32 devices in a mesh: fs: 8 (over z, y), tp: 4 (over x, core).
Axes of the slice: x: 2, y: 2, z: 4, core: 2. Of those that a mesh axis runs over, the one named last changes fastest.
Arguments:
- up_pre: bfloat16 [6144, 4096], P('fs', 'tp'), may hold values from -6 to 6
- gate_value: bfloat16 [6144, 4096], P('fs', 'tp'), may hold values from -6 to 6
- out_cotangent: bfloat16 [6144, 2048], P('fs', 'tp'), may hold values from -8 to 8
- down_weight: bfloat16 [2048, 4096], P('fs', 'tp'), may hold values from -0.09375 to 0.09375
- conv_weight: float32 [3, 4096], P(None, 'tp'), may hold values from -3.5 to 3.5
- conv_bias: float32 [4096], P('tp'), may hold values from -3 to 3
Outputs:
- up_grad: bfloat16 [6144, 4096], P('fs', 'tp')
- gate_grad: bfloat16 [6144, 4096], P('fs', 'tp')
- weight_grad: float32 [2048, 4096], P('fs', 'tp')
- tap_grad: float32 [3, 4096], P(None, 'tp')
- bias_grad: float32 [4096], P('tp')
- unit_norms: float32 [4096], P('tp')
The draws below stay inside these ranges and needn't reach their ends.
All inputs are finite; a program needn't handle non-finite values.
Results may differ from the reference program's by a relative error of at most 0.0034.
Values may be sent and summed in bfloat16 or wider, within the bound.
A program may use at most 64 MiB of HBM per device.

```python
import jax
import jax.numpy as jnp

D = 2048
FF = 4096
TAPS = 3
TOKENS = 6144


def raised(values, stream_key, source, target, shards_of, factor):
    owner, partner = [(jnp.arange(values.shape[position]) // (values.shape[position] // shards_of)).reshape([-1 if axis == position else 1 for axis in range(values.ndim)]) for position in (source, target)]
    chosen = jax.random.permutation(stream_key, shards_of)[partner]
    strong = (owner == chosen) | (owner == (partner + shards_of // 2) % shards_of)
    return jnp.where(strong, factor * values, values)


def level_of(key, dims, shards, least, largest):
    gain = 1.0
    for dim, shards_of in shards:
        heights = jax.random.uniform(jax.random.fold_in(jax.random.fold_in(key, 6), dim), (shards_of,), jnp.float32, least / len(shards), largest / len(shards))
        gain = gain * jnp.repeat(jnp.exp(heights), dims[dim] // shards_of).reshape((-1,) + (1,) * (len(dims) - 1 - dim))
    return gain


def noise(rng, shape, spread, reach, split=(), kind=jnp.bfloat16):
    drawn = spread * jax.random.normal(rng, shape, jnp.float32)
    if split:
        drawn = drawn * level_of(rng, shape, split, -0.22, 0.18)
    return jnp.clip(drawn, -reach, reach).astype(kind)


def heavy_noise(own_key, dims, spread, limit, pieces, heavy, held_as=jnp.bfloat16):
    drawn = spread * jax.random.normal(own_key, dims, jnp.float32)
    if pieces:
        drawn = drawn * level_of(own_key, dims, pieces, -0.22, 0.18)
    return jnp.clip(raised(drawn, jax.random.fold_in(own_key, 3), *heavy), -limit, limit).astype(held_as)


def setup_inputs(seed: int = 0) -> dict:
    seeds = jax.random.split(jax.random.key(seed), 7)
    up_pre = noise(seeds[0], (TOKENS, FF), 1.0, 6.0, ((0, 8), (1, 4)))
    gate_value = noise(seeds[1], (TOKENS, FF), 1.0, 6.0, ((0, 8), (1, 4)))
    out_cotangent = heavy_noise(seeds[2], (TOKENS, D), 1.0, 8.0, ((0, 8), (1, 4)), (0, 1, 8, 2.0))
    down_weight = noise(seeds[3], (D, FF), FF ** -0.5, 0.09375, ((0, 8), (1, 4)))
    conv_weight = noise(seeds[4], (TAPS, FF), TAPS ** -0.5, 3.5, ((1, 4),), jnp.float32)
    conv_bias = noise(seeds[5], (FF,), 0.5, 3.0, ((0, 4),), jnp.float32)
    return dict(up_pre=up_pre, gate_value=gate_value, out_cotangent=out_cotangent, down_weight=down_weight, conv_weight=conv_weight, conv_bias=conv_bias)


def reference(up_pre, gate_value, out_cotangent, down_weight, conv_weight, conv_bias):
    padded = jnp.pad(up_pre.astype(jnp.float32), ((TAPS - 1, 0), (0, 0)))
    conv_out = jnp.zeros((TOKENS, FF), jnp.float32) + conv_bias[None, :]
    for tap_index in range(TAPS):
        conv_out = conv_out + conv_weight[tap_index][None, :] * padded[tap_index:tap_index + TOKENS]
    sigmoid_val = jax.nn.sigmoid(conv_out)
    activated = conv_out * sigmoid_val
    gate_float = gate_value.astype(jnp.float32)
    hidden = (activated * gate_float).astype(jnp.bfloat16)
    hidden_grad = jnp.dot(out_cotangent, down_weight, preferred_element_type=jnp.float32)
    gate_grad = (hidden_grad * activated).astype(jnp.bfloat16)
    conv_grad = hidden_grad * gate_float * sigmoid_val * (1.0 + conv_out * (1.0 - sigmoid_val))
    after = jnp.pad(conv_grad, ((0, TAPS - 1), (0, 0)))
    up_grad = jnp.zeros((TOKENS, FF), jnp.float32)
    for tap_index in range(TAPS):
        lead = TAPS - 1 - tap_index
        up_grad = up_grad + conv_weight[tap_index][None, :] * after[lead:lead + TOKENS]
    tap_grad = jnp.stack([jnp.sum(conv_grad * padded[tap_index:tap_index + TOKENS], axis=0)
                          for tap_index in range(TAPS)])
    bias_grad = jnp.sum(conv_grad, axis=0)
    weight_grad = jnp.dot(out_cotangent.T, hidden, preferred_element_type=jnp.float32)
    unit_norms = jnp.sum(weight_grad * weight_grad, axis=0)
    return (up_grad.astype(jnp.bfloat16), gate_grad, weight_grad, tap_grad, bias_grad, unit_norms)
```

```python
import functools

import jax
import jax.numpy as jnp
from jax import lax
from jax.experimental import pallas as pl
from jax.experimental.pallas import tpu as pltpu
from jax.sharding import PartitionSpec as P

MESH = pl.DeviceIdType.MESH
F32 = jnp.float32
BF16 = jnp.bfloat16


def kernel(
    fs_n, tp_n, y_n,
    up_hbm, gate_hbm, cot_ref, w_ref, cw_hbm, cb_hbm,
    ug_ref, gg_ref, wg_ref, tap_ref, bias_ref, norm_ref,
    wfull, cotf, lhs_t, hidden, act, gfac, upf, cg, pf32, pbf,
    r1, s2, r2, st, nb, halo_up, halo_cg, up_ref, gate_ref, cw_ref, cb_ref,
    local_sem, w_recv, w_send_z, w_send_y, c_recv, c_send_x, c_send_m,
    r1_recv, r1_send, r2_recv, r2_send, st_recv, st_send, nb_recv, nb_send,
    hu_sem, hc_sem,
):
    rows, cols = up_hbm.shape
    dblk = w_ref.shape[0]
    cshard = cot_ref.shape[1]
    z_n = fs_n // y_n
    x_n = tp_n // 2
    me, tp = lax.axis_index("fs"), lax.axis_index("tp")
    mz, my = me // y_n, me % y_n
    mx, mc = tp // 2, tp % 2
    mate = mx * 2 + (1 - mc)
    sends = []

    def rcopy(src, dst, ss, rs, fs_id, tp_id):
        return pltpu.make_async_remote_copy(
            src_ref=src, dst_ref=dst, send_sem=ss, recv_sem=rs,
            device_id=(fs_id, tp_id), device_id_type=MESH,
        )

    def send(*args):
        copy = rcopy(*args)
        copy.start()
        sends.append(copy)

    def wrows(owner):
        return wfull.at[pl.ds(pl.multiple_of(owner * dblk, dblk), dblk)]

    def ccols(owner):
        return cotf.at[:, pl.ds(pl.multiple_of(owner * cshard, cshard), cshard)]

    own_w = pltpu.make_async_copy(w_ref, wrows(me), local_sem.at[0])
    own_c = pltpu.make_async_copy(cot_ref, ccols(tp), local_sem.at[1])
    loads = [
        pltpu.make_async_copy(src, dst, local_sem.at[k])
        for k, (src, dst) in enumerate(
            [(up_hbm, up_ref), (gate_hbm, gate_ref), (cw_hbm, cw_ref), (cb_hbm, cb_ref)], 2
        )
    ]

    barrier = pltpu.get_barrier_semaphore()
    peers = [((me + d) % fs_n, tp) for d in range(1, fs_n)]
    peers += [(me, ((mx + d) % x_n) * 2 + mc) for d in range(1, x_n)] + [(me, mate)]
    for peer in peers:
        pl.semaphore_signal(barrier, inc=1, device_id=peer, device_id_type=MESH)
    for copy in loads:
        copy.start()
    pl.semaphore_wait(barrier, len(peers))

    @pl.when(me < fs_n - 1)
    def _():
        rcopy(up_hbm.at[pl.ds(rows - 16, 16)], halo_up, hu_sem.at[0], hu_sem.at[1], me + 1, tp).start()

    for d in range(1, x_n):
        send(cot_ref, ccols(tp), c_send_x.at[d], c_recv.at[tp], me, ((mx + d) % x_n) * 2 + mc)
    for d in range(1, z_n):
        send(w_ref, wrows(me), w_send_z.at[d], w_recv.at[me], ((mz + d) % z_n) * y_n + my, tp)
    for d in range(1, y_n):
        send(w_ref, wrows(me), w_send_y.at[d], w_recv.at[me], mz * y_n + (my + d) % y_n, tp)
    send(cot_ref, ccols(tp), c_send_m.at[0], c_recv.at[tp], me, mate)
    own_w.start()
    own_c.start()

    for copy in loads:
        copy.wait()

    @pl.when(me > 0)
    def _():
        rcopy(halo_up, halo_up, hu_sem.at[0], hu_sem.at[1], me - 1, tp).wait_recv()
        upf[0:8] = halo_up[...].astype(F32)[8:16]

    @pl.when(me == 0)
    def _():
        upf[0:8] = jnp.zeros((8, cols), F32)

    upf[8 : rows + 8] = up_ref[...].astype(F32)
    step = 64

    @pl.loop(0, cols // 128)
    def _(j):
        lanes = pl.ds(pl.multiple_of(j * 128, 128), 128)
        taps = [cw_ref[k : k + 1, lanes] for k in range(3)]
        bias = cb_ref[0:1, lanes]
        for r in range(0, rows, step):
            conv = bias + taps[0] * upf[r + 6 : r + 6 + step, lanes]
            conv = conv + taps[1] * upf[r + 7 : r + 7 + step, lanes]
            conv = conv + taps[2] * upf[r + 8 : r + 8 + step, lanes]
            sig = 1.0 / (1.0 + jnp.exp(-conv))
            a = conv * sig
            g = gate_ref[r : r + step, lanes].astype(F32)
            act[r : r + step, lanes] = a
            hidden[r : r + step, lanes] = (a * g).astype(BF16)
            gfac[r : r + step, lanes] = g * sig * (1.0 + conv * (1.0 - sig))

    def wait_cot(d, other):
        owner = ((mx + x_n - d) % x_n) * 2 + (1 - mc if other else mc)
        sem = c_send_m if other else c_send_x
        rcopy(cot_ref, ccols(owner), sem.at[d], c_recv.at[owner], me, mate if other else owner).wait_recv()
        return owner

    ywide = y_n * dblk
    tile = min(256, cols)
    own_chunks = max(z_n // x_n, 1)

    def chunk(o):
        return (mx * own_chunks + o) % z_n

    def partial_grad(o):
        zp = chunk(o)
        base = pl.multiple_of(zp * ywide, ywide)
        lhs_t[...] = cotf[:, pl.ds(base, ywide)].T

        @pl.loop(0, cols // tile)
        def _(j):
            lanes = pl.ds(pl.multiple_of(j * tile, tile), tile)
            out = jnp.dot(lhs_t[...], hidden[:, lanes], preferred_element_type=F32)
            pf32[pl.ds(base, ywide), lanes] = out
            pbf[pl.ds(base, ywide), lanes] = out.astype(BF16)

        for e in range(1, y_n):
            yp = (my + e) % y_n
            block = pl.ds(pl.multiple_of((zp * y_n + yp) * dblk, dblk), dblk)
            sem = (e - 1) * z_n + o
            send(pbf.at[block], r1.at[e - 1, o], r1_send.at[sem], r1_recv.at[sem], mz * y_n + yp, tp)

    own_c.wait()
    wait_cot(0, True)
    for o in range(own_chunks):
        partial_grad(o)
    for d in range(1, x_n):
        owner = wait_cot(d, False)
        send(ccols(owner), ccols(owner), c_send_m.at[d], c_recv.at[owner], me, mate)
    for d in range(1, x_n):
        wait_cot(d, True)
    for o in range(own_chunks, z_n):
        partial_grad(o)

    def y_sum_wait(o):
        for e in range(1, y_n):
            sem = (e - 1) * z_n + o
            rcopy(r1.at[e - 1, o], r1.at[e - 1, o], r1_send.at[sem], r1_recv.at[sem],
                  mz * y_n + (my + e) % y_n, tp).wait_recv()

    def y_sum(o, block, lanes):
        total = pf32[block, lanes]
        for e in range(1, y_n):
            total = total + r1[e - 1, o, :, lanes].astype(F32)
        return total

    def z_copy(o):
        return rcopy(s2.at[o], r2.at[mz], r2_send.at[o], r2_recv.at[mz], chunk(o) * y_n + my, tp)

    def sum_and_send(o):
        zp = chunk(o)
        block = pl.ds(pl.multiple_of((zp * y_n + my) * dblk, dblk), dblk)
        y_sum_wait(o)

        @pl.when(zp != mz)
        def _():
            @pl.loop(0, cols // 128)
            def _(j):
                lanes = pl.ds(pl.multiple_of(j * 128, 128), 128)
                s2[o, :, lanes] = y_sum(o, block, lanes).astype(BF16)

            z_copy(o).start()

    early = z_n // 2
    for o in range(early):
        sum_and_send(o)

    own_w.wait()
    for d in range(1, z_n):
        owner = ((mz + z_n - d) % z_n) * y_n + my
        rcopy(w_ref, wrows(owner), w_send_z.at[d], w_recv.at[owner], owner, tp).wait_recv()
        for e in range(1, y_n):
            send(wrows(owner), wrows(owner), w_send_y.at[d * y_n + e], w_recv.at[owner],
                 mz * y_n + (my + e) % y_n, tp)

    part_rows = 256

    def add_block(owner, first, last):
        wide = pl.multiple_of(owner * dblk, dblk)

        @pl.loop(0, cols // tile)
        def _(j):
            lanes = pl.ds(pl.multiple_of(j * tile, tile), tile)

            @pl.loop(0, rows // part_rows)
            def _(i):
                part = pl.ds(pl.multiple_of(i * part_rows, part_rows), part_rows)
                hg = jnp.dot(cotf[part, pl.ds(wide, dblk)], wfull[pl.ds(wide, dblk), lanes], preferred_element_type=F32)
                if not first:
                    hg = hg + cg[part, lanes]
                if last:
                    gg_ref[part, lanes] = (hg * act[part, lanes]).astype(BF16)
                    hg = hg * gfac[part, lanes]
                cg[part, lanes] = hg

    sum_and_send(early)
    small = dblk % 128 != 0
    if not small:
        for d in range(z_n):
            add_block(((mz + z_n - d) % z_n) * y_n + my, d == 0, False)
    for o in range(early + 1, z_n):
        sum_and_send(o)
    for d in range(z_n):
        for e in range(1, y_n):
            owner = ((mz + z_n - d) % z_n) * y_n + (my + y_n - e) % y_n
            rcopy(wrows(owner), wrows(owner), w_send_y.at[d * y_n + e], w_recv.at[owner],
                  mz * y_n + (my + e) % y_n, tp).wait_recv()
            if not small:
                add_block(owner, False, d == z_n - 1 and e == y_n - 1)
    if small:

        @pl.loop(0, cols // tile)
        def _(j):
            lanes = pl.ds(pl.multiple_of(j * tile, tile), tile)

            @pl.loop(0, rows // part_rows)
            def _(i):
                part = pl.ds(pl.multiple_of(i * part_rows, part_rows), part_rows)
                hg = jnp.dot(cotf[part, :], wfull[:, lanes], preferred_element_type=F32)
                gg_ref[part, lanes] = (hg * act[part, lanes]).astype(BF16)
                cg[part, lanes] = hg * gfac[part, lanes]

    @pl.when(me > 0)
    def _():
        rcopy(cg.at[pl.ds(0, 8)], halo_cg, hc_sem.at[0], hc_sem.at[1], me - 1, tp).start()

    @pl.loop(0, cols // 128)
    def _(j):
        lanes = pl.ds(pl.multiple_of(j * 128, 128), 128)
        sums = [jnp.zeros((8, 128), F32) for _ in range(4)]
        for r in range(0, rows, step):
            grad = cg[r : r + step, lanes]
            terms = [grad * upf[r + 6 + k : r + 6 + k + step, lanes] for k in range(3)] + [grad]
            sums = [s + jnp.sum(t.reshape(step // 8, 8, 128), axis=0) for s, t in zip(sums, terms)]
        for k in range(4):
            st[me, k : k + 1, lanes] = jnp.sum(sums[k], axis=0, keepdims=True)
        st[me, 4:8, lanes] = jnp.zeros((4, 128), F32)

    for d in range(1, fs_n):
        send(st.at[me], st.at[me], st_send.at[d], st_recv.at[me], (me + d) % fs_n, tp)

    mine = (mz + z_n - chunk(0)) % z_n
    for d in range(1, z_n):
        zp = (mz + d) % z_n
        rcopy(s2.at[0], r2.at[zp], r2_send.at[0], r2_recv.at[zp], zp * y_n + my, tp).wait_recv()
    own_block = pl.ds(pl.multiple_of(me * dblk, dblk), dblk)

    @pl.loop(0, cols // 128)
    def _(j):
        lanes = pl.ds(pl.multiple_of(j * 128, 128), 128)
        total = y_sum(mine, own_block, lanes)
        for d in range(1, z_n):
            total = total + r2[(mz + d) % z_n, :, lanes].astype(F32)
        wg_ref[:, lanes] = total
        nb[me, :, lanes] = jnp.sum(total * total, axis=0, keepdims=True)

    for d in range(1, fs_n):
        send(nb.at[me], nb.at[me], nb_send.at[d], nb_recv.at[me], (me + d) % fs_n, tp)

    @pl.when(me < fs_n - 1)
    def _():
        rcopy(halo_cg, halo_cg, hc_sem.at[0], hc_sem.at[1], me + 1, tp).wait_recv()
        cg[rows : rows + 8] = halo_cg[...]

    @pl.when(me == fs_n - 1)
    def _():
        cg[rows : rows + 8] = jnp.zeros((8, cols), F32)

    @pl.loop(0, cols // 128)
    def _(j):
        lanes = pl.ds(pl.multiple_of(j * 128, 128), 128)
        taps = [cw_ref[k : k + 1, lanes] for k in range(3)]
        for r in range(0, rows, step):
            total = taps[0] * cg[r + 2 : r + 2 + step, lanes]
            total = total + taps[1] * cg[r + 1 : r + 1 + step, lanes]
            total = total + taps[2] * cg[r : r + step, lanes]
            ug_ref[r : r + step, lanes] = total.astype(BF16)

    for d in range(1, fs_n):
        owner = (me + d) % fs_n
        rcopy(st.at[owner], st.at[owner], st_send.at[d], st_recv.at[owner], owner, tp).wait_recv()
    stats = st[0]
    for k in range(1, fs_n):
        stats = stats + st[k]
    tap_ref[...] = stats[0:3]
    bias_ref[...] = stats[3:4]
    for d in range(1, fs_n):
        owner = (me + d) % fs_n
        rcopy(nb.at[owner], nb.at[owner], nb_send.at[d], nb_recv.at[owner], owner, tp).wait_recv()
    norms = nb[0]
    for k in range(1, fs_n):
        norms = norms + nb[k]
    norm_ref[...] = norms

    for copy in sends:
        copy.wait_send()
    for o in range(z_n):

        @pl.when(chunk(o) != mz)
        def _():
            z_copy(o).wait_send()

    @pl.when(me < fs_n - 1)
    def _():
        rcopy(up_hbm.at[pl.ds(rows - 16, 16)], halo_up, hu_sem.at[0], hu_sem.at[1], me + 1, tp).wait_send()

    @pl.when(me > 0)
    def _():
        rcopy(cg.at[pl.ds(0, 8)], halo_cg, hc_sem.at[0], hc_sem.at[1], me - 1, tp).wait_send()


def general_call(fs_n, tp_n, y_n, args):
    up_pre, _, _, down_weight, _, _ = args
    rows, cols = up_pre.shape
    dblk = down_weight.shape[0]
    width = dblk * fs_n
    z_n = fs_n // y_n
    dma = pltpu.SemaphoreType.DMA
    vmem = pl.BlockSpec(memory_space=pltpu.VMEM)
    return pl.pallas_call(
        functools.partial(kernel, fs_n, tp_n, y_n),
        out_shape=(
            jax.ShapeDtypeStruct((rows, cols), BF16),
            jax.ShapeDtypeStruct((rows, cols), BF16),
            jax.ShapeDtypeStruct((dblk, cols), F32),
            jax.ShapeDtypeStruct((3, cols), F32),
            jax.ShapeDtypeStruct((1, cols), F32),
            jax.ShapeDtypeStruct((1, cols), F32),
        ),
        in_specs=[pl.BlockSpec(memory_space=pltpu.HBM)] * 6,
        out_specs=[vmem] * 6,
        scratch_shapes=[
            pltpu.VMEM((width, cols), BF16),
            pltpu.VMEM((rows, width), BF16),
            pltpu.VMEM((y_n * dblk, rows), BF16),
            pltpu.VMEM((rows, cols), BF16),
            pltpu.VMEM((rows, cols), F32),
            pltpu.VMEM((rows, cols), F32),
            pltpu.VMEM((rows + 8, cols), F32),
            pltpu.VMEM((rows + 8, cols), F32),
            pltpu.VMEM((width, cols), F32),
            pltpu.VMEM((width, cols), BF16),
            pltpu.VMEM((y_n - 1, z_n, dblk, cols), BF16),
            pltpu.VMEM((z_n, dblk, cols), BF16),
            pltpu.VMEM((z_n, dblk, cols), BF16),
            pltpu.VMEM((fs_n, 8, cols), F32),
            pltpu.VMEM((fs_n, 1, cols), F32),
            pltpu.VMEM((16, cols), BF16),
            pltpu.VMEM((8, cols), F32),
            pltpu.VMEM((rows, cols), BF16),
            pltpu.VMEM((rows, cols), BF16),
            pltpu.VMEM((3, cols), F32),
            pltpu.VMEM((1, cols), F32),
            dma((6,)),
            dma((fs_n,)), dma((z_n,)), dma((z_n * y_n,)),
            dma((tp_n,)), dma((tp_n // 2,)), dma((tp_n // 2,)),
            dma(((y_n - 1) * z_n,)), dma(((y_n - 1) * z_n,)),
            dma((z_n,)), dma((z_n,)),
            dma((fs_n,)), dma((fs_n,)), dma((fs_n,)), dma((fs_n,)),
            dma((2,)), dma((2,)),
        ],
        compiler_params=pltpu.CompilerParams(
            collective_id=0, has_side_effects=True, vmem_limit_bytes=48000 * 1024
        ),
    )(*args)


def line_kernel(
    fs_n, tp_n, y_n, n1,
    up_hbm, gate_hbm, cot_hbm, w_hbm, cw_hbm, cb_hbm,
    ug_ref, gg_ref, wg_ref, tap_ref, bias_ref, norm_ref,
    wfull, cotf, lhs_t, hidden, act, gfac, upf, cg, pf32,
    ysend, yrecv, sz1, rz1, sz2, rz2, sf, rf,
    st, nb, halo_up, halo_cg, up_ref, gate_ref, cw_ref, cb_ref,
    local_sem, ag_send, ag_recv, yw_send, yw_recv, yp_sem, c_send, c_recv, ry_send, ry_recv,
    rs_send, rs_recv, f_sem, st_recv, st_send, nb_recv, nb_send, hu_sem, hc_sem,
):
    rows, cols = up_hbm.shape
    dblk = w_hbm.shape[0]
    cshard = cot_hbm.shape[1]
    ywide = y_n * dblk
    z_n = fs_n // y_n
    n2 = cols - n1
    me, tp = lax.axis_index("fs"), lax.axis_index("tp")
    mz, my = me // y_n, me % y_n
    mx, mc = tp // 2, tp % 2
    mate = mx * 2 + (1 - mc)
    mirror = (1 - mx) * 2 + mc
    across = (1 - mx) * 2 + (1 - mc)
    ynb = mz * y_n + (1 - my)
    sign = (1, -1)
    avail = (mz, z_n - 1 - mz)
    has_next = (mz < z_n - 1, mz > 0)
    has_prev = (mz > 0, mz < z_n - 1)
    nxt = [((mz + z_n + s) % z_n) * y_n + my for s in sign]
    sends = []

    def rcopy(src, dst, ss, rs, fs_id, tp_id):
        return pltpu.make_async_remote_copy(
            src_ref=src, dst_ref=dst, send_sem=ss, recv_sem=rs,
            device_id=(fs_id, tp_id), device_id_type=MESH,
        )

    def start(make, pred=None, inside=None):
        if pred is None:
            make().start()
        else:
            @pl.when(pred if inside is None else inside)
            def _():
                make().start()
        sends.append((pred, make))

    def drows(zp, y):
        return pl.ds(pl.multiple_of((zp * y_n + y) * dblk, dblk), dblk)

    def ccols(owner):
        return cotf.at[:, pl.ds(pl.multiple_of(owner * cshard, cshard), cshard)]

    part1, part2 = pl.ds(0, n1), pl.ds(n1, n2)

    def ag_copy(d, slot, part, zp):
        ref = wfull.at[drows(zp, 1 - my if part == 2 else my), part1 if part == 1 else part2]
        src = ref
        if slot == 0 and part < 2:
            src = w_hbm.at[:, part1 if part == 1 else part2]
        i = (d * z_n + slot) * 3 + part
        return rcopy(src, ref, ag_send.at[i], ag_recv.at[i], nxt[d], tp)

    def yw_copy(zp, own=False):
        ref = wfull.at[drows(zp, my), part1]
        return rcopy(w_hbm.at[:, part1] if own else ref, ref, yw_send.at[zp], yw_recv.at[zp], ynb, tp)

    def yw_wait(zp):
        ref = wfull.at[drows(zp, 1 - my), part1]
        rcopy(ref, ref, yw_send.at[zp], yw_recv.at[zp], ynb, tp).wait_recv()

    def rs_copy(d, slot, part, t):
        i = (d * z_n + slot) * 2 + part
        src, dst = (sz2.at[t], rz2.at[d, t]) if part == 0 else (sz1.at[t], rz1.at[d, t])
        return rcopy(src, dst, rs_send.at[i], rs_recv.at[i], nxt[d], tp)

    def ry_copy(t):
        return rcopy(ysend.at[t], yrecv.at[t], ry_send.at[t], ry_recv.at[t], ynb, tp)

    own_w = pltpu.make_async_copy(w_hbm, wfull.at[drows(mz, my)], local_sem.at[0])
    own_c = pltpu.make_async_copy(cot_hbm, ccols(tp), local_sem.at[1])
    loads = [
        pltpu.make_async_copy(src, dst, local_sem.at[k])
        for k, (src, dst) in enumerate(
            [(up_hbm, up_ref), (gate_hbm, gate_ref), (cw_hbm, cw_ref), (cb_hbm, cb_ref)], 2
        )
    ]

    barrier = pltpu.get_barrier_semaphore()
    peers = [((me + d) % fs_n, tp) for d in range(1, fs_n)] + [(me, mirror), (me, mate)]
    for peer in peers:
        pl.semaphore_signal(barrier, inc=1, device_id=peer, device_id_type=MESH)
    for copy in loads:
        copy.start()
    own_c.start()
    own_w.start()
    pl.semaphore_wait(barrier, len(peers))

    start(
        lambda: rcopy(up_hbm.at[pl.ds(rows - 16, 16)], halo_up, hu_sem.at[0], hu_sem.at[1], (me + 1) % fs_n, tp),
        me < fs_n - 1,
    )
    yp_copy = lambda: rcopy(
        w_hbm.at[:, part2], wfull.at[drows(mz, my), part2], yp_sem.at[0], yp_sem.at[1], ynb, tp
    )
    start(yp_copy)
    for part in (0, 1):
        for d in (0, 1):
            start(functools.partial(ag_copy, d, 0, part, mz), has_next[d])
    start(functools.partial(yw_copy, mz, True))
    start(lambda: rcopy(cot_hbm, ccols(tp), c_send.at[0], c_recv.at[tp], me, mirror))
    start(lambda: rcopy(cot_hbm, ccols(tp), c_send.at[1], c_recv.at[tp], me, mate))

    for copy in loads:
        copy.wait()

    @pl.when(me > 0)
    def _():
        rcopy(halo_up, halo_up, hu_sem.at[0], hu_sem.at[1], (me + fs_n - 1) % fs_n, tp).wait_recv()
        upf[0:8] = halo_up[...].astype(F32)[8:16]

    @pl.when(me == 0)
    def _():
        upf[0:8] = jnp.zeros((8, cols), F32)

    upf[8 : rows + 8] = up_ref[...].astype(F32)
    step = 64

    @pl.loop(0, cols // 128)
    def _(j):
        lanes = pl.ds(pl.multiple_of(j * 128, 128), 128)
        taps = [cw_ref[k : k + 1, lanes] for k in range(3)]
        bias = cb_ref[0:1, lanes]
        for r in range(0, rows, step):
            conv = bias + taps[0] * upf[r + 6 : r + 6 + step, lanes]
            conv = conv + taps[1] * upf[r + 7 : r + 7 + step, lanes]
            conv = conv + taps[2] * upf[r + 8 : r + 8 + step, lanes]
            sig = 1.0 / (1.0 + jnp.exp(-conv))
            a = conv * sig
            g = gate_ref[r : r + step, lanes].astype(F32)
            act[r : r + step, lanes] = a
            hidden[r : r + step, lanes] = (a * g).astype(BF16)
            gfac[r : r + step, lanes] = g * sig * (1.0 + conv * (1.0 - sig))

    rcopy(
        w_hbm.at[:, part2], wfull.at[drows(mz, 1 - my), part2], yp_sem.at[0], yp_sem.at[1], ynb, tp
    ).wait_recv()
    for d in (0, 1):
        start(functools.partial(ag_copy, d, 0, 2, mz), has_next[d])

    tile = min(256, cols)

    def wg_part(t):
        base = pl.multiple_of(t * ywide, ywide)
        lhs_t[...] = cotf[:, pl.ds(base, ywide)].T

        @pl.loop(0, cols // tile)
        def _(j):
            lanes = pl.ds(pl.multiple_of(j * tile, tile), tile)
            pf32[pl.ds(base, ywide), lanes] = jnp.dot(lhs_t[...], hidden[:, lanes], preferred_element_type=F32)

        @pl.loop(0, n1 // 128)
        def _(j):
            lanes = pl.ds(pl.multiple_of(j * 128, 128), 128)
            ysend[t, :, lanes] = pf32[drows(t, 1 - my), lanes].astype(BF16)

    def wg_half(half):
        low = half * (z_n // 2)
        first = jnp.where(half == 0, jnp.where(mz == 0, 1, 0), jnp.where(mz == z_n - 1, 0, 1))
        wg_part(low + first)
        wg_part(low + 1 - first)

    def ry_start(delta, half=None):
        for s in sign if delta else (1,):
            t = mz + s * delta
            pred = (t >= 0) & (t < z_n)
            t = (t + z_n) % z_n
            if half is not None:
                pred = pred & (t // (z_n // 2) == half)
            start(functools.partial(ry_copy, t), pred)

    own_c.wait()
    rcopy(cot_hbm, ccols(mate), c_send.at[1], c_recv.at[mate], me, mate).wait_recv()
    wg_half(mx)
    ry_start(z_n - 1, mx)

    def ag_step(k):
        for d in (0, 1):
            zp = (mz + z_n - sign[d] * (1 + k)) % z_n
            is_ag = k < avail[d]
            fwd = is_ag & has_next[d]

            @pl.when(is_ag)
            def _():
                for part in (0, 1, 2):
                    ag_copy(d, k, part, zp).wait_recv()
                    if k + 1 < z_n - 1:
                        @pl.when(has_next[d])
                        def _():
                            ag_copy(d, k + 1, part, zp).start()
                    if part == 1:
                        yw_copy(zp).start()

            for part in (0, 1, 2):
                if k + 1 < z_n - 1:
                    sends.append((fwd, functools.partial(ag_copy, d, k + 1, part, zp)))
            sends.append((is_ag, functools.partial(yw_copy, zp)))

    def rs_step(k):
        for d in (0, 1):
            t = (mz + z_n - sign[d] * (1 + k)) % z_n
            pred = k >= avail[d]

            def run(arrived, d=d, t=t):
                if arrived:
                    rs_copy(d, k, 0, t).wait_recv()

                @pl.loop(0, n2 // 128)
                def _(j):
                    far = pl.ds(pl.multiple_of(n1 + j * 128, 128), 128)
                    near = pl.ds(pl.multiple_of(j * 128, 128), 128)
                    total = pf32[pl.ds(pl.multiple_of(t * ywide, ywide), ywide), far]
                    if arrived:
                        total = total + rz2[d, t, :, near].astype(F32)
                    sz2[t, :, near] = total.astype(BF16)

                rs_copy(d, k + 1, 0, t).start()
                ry_copy(t).wait_recv()
                if arrived:
                    rs_copy(d, k, 1, t).wait_recv()

                @pl.loop(0, n1 // 128)
                def _(j):
                    lanes = pl.ds(pl.multiple_of(j * 128, 128), 128)
                    total = pf32[drows(t, my), lanes] + yrecv[t, :, lanes].astype(F32)
                    if arrived:
                        total = total + rz1[d, t, :, lanes].astype(F32)
                    sz1[t, :, lanes] = total.astype(BF16)

                rs_copy(d, k + 1, 1, t).start()

            if k > 0:
                pl.when(pred & has_prev[d])(functools.partial(run, True))
            pl.when(pred & jnp.logical_not(has_prev[d]))(functools.partial(run, False))
            for part in (0, 1):
                sends.append((pred, functools.partial(rs_copy, d, k + 1, part, t)))

    part_rows = rows // 2 if rows % 32 == 0 else rows

    def hg_add(zp, first):
        base = pl.ds(pl.multiple_of(zp * ywide, ywide), ywide)

        @pl.loop(0, cols // tile)
        def _(j):
            lanes = pl.ds(pl.multiple_of(j * tile, tile), tile)

            @pl.loop(0, rows // part_rows)
            def _(i):
                part = pl.ds(pl.multiple_of(i * part_rows, part_rows), part_rows)
                hg = jnp.dot(cotf[part, base], wfull[base, lanes], preferred_element_type=F32)
                if not first:
                    hg = hg + cg[part, lanes]
                cg[part, lanes] = hg

    def hg_far(delta):
        for s in sign:
            zp = mz + s * delta

            @pl.when((zp >= 0) & (zp < z_n))
            def _():
                near = (zp + z_n) % z_n
                yw_wait(near)
                hg_add(near, False)

    ag_step(0)
    rcopy(cot_hbm, ccols(mirror), c_send.at[0], c_recv.at[mirror], me, mirror).wait_recv()
    start(lambda: rcopy(ccols(mirror), ccols(mirror), c_send.at[2], c_recv.at[mirror], me, mate))
    rcopy(cot_hbm, ccols(across), c_send.at[2], c_recv.at[across], me, mate).wait_recv()
    wg_half(1 - mx)
    ry_start(z_n - 1, 1 - mx)
    for delta in range(z_n - 2, 1, -1):
        ry_start(delta)
    rs_step(0)
    own_w.wait()
    yw_wait(mz)
    hg_add(mz, True)
    for k in range(1, z_n - 1):
        ag_step(k)
        if k == 1:
            ry_start(1)
        if k == z_n - 2:
            ry_start(0)
        rs_step(k)
        hg_far(k)
    hg_far(z_n - 1)

    @pl.loop(0, cols // 128)
    def _(j):
        lanes = pl.ds(pl.multiple_of(j * 128, 128), 128)
        for r in range(0, rows, step):
            part = slice(r, r + step)
            hg = cg[part, lanes]
            gg_ref[part, lanes] = (hg * act[part, lanes]).astype(BF16)
            cg[part, lanes] = hg * gfac[part, lanes]

    start(
        lambda: rcopy(cg.at[pl.ds(0, 8)], halo_cg, hc_sem.at[0], hc_sem.at[1], (me + fs_n - 1) % fs_n, tp),
        me > 0,
    )

    @pl.loop(0, cols // 128)
    def _(j):
        lanes = pl.ds(pl.multiple_of(j * 128, 128), 128)
        sums = [jnp.zeros((8, 128), F32) for _ in range(4)]
        for r in range(0, rows, step):
            grad = cg[r : r + step, lanes]
            terms = [grad * upf[r + 6 + k : r + 6 + k + step, lanes] for k in range(3)] + [grad]
            sums = [s + jnp.sum(t.reshape(step // 8, 8, 128), axis=0) for s, t in zip(sums, terms)]
        for k in range(4):
            st[me, k : k + 1, lanes] = jnp.sum(sums[k], axis=0, keepdims=True)

    for d in range(1, fs_n):
        start(
            lambda d=d: rcopy(st.at[me], st.at[me], st_send.at[d], st_recv.at[me], (me + d) % fs_n, tp)
        )

    last = z_n - 1
    for d in (0, 1):

        @pl.when(has_prev[d])
        def _():
            rs_copy(d, last, 0, mz).wait_recv()

            @pl.loop(0, n2 // 128)
            def _(j):
                far = pl.ds(pl.multiple_of(n1 + j * 128, 128), 128)
                near = pl.ds(pl.multiple_of(j * 128, 128), 128)
                block = pl.ds(pl.multiple_of(mz * ywide, ywide), ywide)
                pf32[block, far] = pf32[block, far] + rz2[d, mz, :, near].astype(F32)

    @pl.loop(0, n2 // 128)
    def _(j):
        far = pl.ds(pl.multiple_of(n1 + j * 128, 128), 128)
        near = pl.ds(pl.multiple_of(j * 128, 128), 128)
        sf[:, near] = pf32[drows(mz, 1 - my), far].astype(BF16)

    f_copy = lambda: rcopy(sf, rf, f_sem.at[0], f_sem.at[1], ynb, tp)
    start(f_copy)

    @pl.when(me < fs_n - 1)
    def _():
        rcopy(halo_cg, halo_cg, hc_sem.at[0], hc_sem.at[1], (me + 1) % fs_n, tp).wait_recv()
        cg[rows : rows + 8] = halo_cg[...]

    @pl.when(me == fs_n - 1)
    def _():
        cg[rows : rows + 8] = jnp.zeros((8, cols), F32)

    @pl.loop(0, cols // 128)
    def _(j):
        lanes = pl.ds(pl.multiple_of(j * 128, 128), 128)
        taps = [cw_ref[k : k + 1, lanes] for k in range(3)]
        for r in range(0, rows, step):
            total = taps[0] * cg[r + 2 : r + 2 + step, lanes]
            total = total + taps[1] * cg[r + 1 : r + 1 + step, lanes]
            total = total + taps[2] * cg[r : r + step, lanes]
            ug_ref[r : r + step, lanes] = total.astype(BF16)

    own_block = drows(mz, my)
    ry_copy(mz).wait_recv()

    @pl.loop(0, n1 // 128)
    def _(j):
        lanes = pl.ds(pl.multiple_of(j * 128, 128), 128)
        wg_ref[:, lanes] = pf32[own_block, lanes] + yrecv[mz, :, lanes].astype(F32)

    for d in (0, 1):

        @pl.when(has_prev[d])
        def _():
            rs_copy(d, last, 1, mz).wait_recv()

            @pl.loop(0, n1 // 128)
            def _(j):
                lanes = pl.ds(pl.multiple_of(j * 128, 128), 128)
                wg_ref[:, lanes] = wg_ref[:, lanes] + rz1[d, mz, :, lanes].astype(F32)

    f_copy().wait_recv()

    @pl.loop(0, n2 // 128)
    def _(j):
        far = pl.ds(pl.multiple_of(n1 + j * 128, 128), 128)
        near = pl.ds(pl.multiple_of(j * 128, 128), 128)
        wg_ref[:, far] = pf32[own_block, far] + rf[:, near].astype(F32)

    @pl.loop(0, cols // 128)
    def _(j):
        lanes = pl.ds(pl.multiple_of(j * 128, 128), 128)
        total = wg_ref[:, lanes]
        nb[me, :, lanes] = jnp.sum(total * total, axis=0, keepdims=True)

    for d in range(1, fs_n):
        start(
            lambda d=d: rcopy(nb.at[me], nb.at[me], nb_send.at[d], nb_recv.at[me], (me + d) % fs_n, tp)
        )

    for d in range(1, fs_n):
        owner = (me + d) % fs_n
        rcopy(st.at[owner], st.at[owner], st_send.at[d], st_recv.at[owner], owner, tp).wait_recv()
    stats = st[0]
    for k in range(1, fs_n):
        stats = stats + st[k]
    tap_ref[...] = stats[0:3]
    bias_ref[...] = stats[3:4]

    for pred, make in sends:
        if pred is None:
            make().wait_send()
        else:
            @pl.when(pred)
            def _():
                make().wait_send()

    for d in range(1, fs_n):
        owner = (me + d) % fs_n
        rcopy(nb.at[owner], nb.at[owner], nb_send.at[d], nb_recv.at[owner], owner, tp).wait_recv()
    norms = nb[0]
    for k in range(1, fs_n):
        norms = norms + nb[k]
    norm_ref[...] = norms


def line_call(fs_n, tp_n, y_n, args):
    up_pre, _, _, down_weight, _, _ = args
    rows, cols = up_pre.shape
    dblk = down_weight.shape[0]
    width = dblk * fs_n
    ywide = y_n * dblk
    z_n = fs_n // y_n
    n2 = max(cols * 3 // 8 // 128, 1) * 128
    n1 = cols - n2
    dma = pltpu.SemaphoreType.DMA
    vmem = pl.BlockSpec(memory_space=pltpu.VMEM)
    return pl.pallas_call(
        functools.partial(line_kernel, fs_n, tp_n, y_n, n1),
        out_shape=(
            jax.ShapeDtypeStruct((rows, cols), BF16),
            jax.ShapeDtypeStruct((rows, cols), BF16),
            jax.ShapeDtypeStruct((dblk, cols), F32),
            jax.ShapeDtypeStruct((3, cols), F32),
            jax.ShapeDtypeStruct((1, cols), F32),
            jax.ShapeDtypeStruct((1, cols), F32),
        ),
        in_specs=[pl.BlockSpec(memory_space=pltpu.HBM)] * 6,
        out_specs=[vmem] * 6,
        scratch_shapes=[
            pltpu.VMEM((width, cols), BF16),
            pltpu.VMEM((rows, width), BF16),
            pltpu.VMEM((ywide, rows), BF16),
            pltpu.VMEM((rows, cols), BF16),
            pltpu.VMEM((rows, cols), F32),
            pltpu.VMEM((rows, cols), F32),
            pltpu.VMEM((rows + 8, cols), F32),
            pltpu.VMEM((rows + 8, cols), F32),
            pltpu.VMEM((width, cols), F32),
            pltpu.VMEM((z_n, dblk, n1), BF16),
            pltpu.VMEM((z_n, dblk, n1), BF16),
            pltpu.VMEM((z_n, dblk, n1), BF16),
            pltpu.VMEM((2, z_n, dblk, n1), BF16),
            pltpu.VMEM((z_n, ywide, n2), BF16),
            pltpu.VMEM((2, z_n, ywide, n2), BF16),
            pltpu.VMEM((dblk, n2), BF16),
            pltpu.VMEM((dblk, n2), BF16),
            pltpu.VMEM((fs_n, 4, cols), F32),
            pltpu.VMEM((fs_n, 1, cols), F32),
            pltpu.VMEM((16, cols), BF16),
            pltpu.VMEM((8, cols), F32),
            pltpu.VMEM((rows, cols), BF16),
            pltpu.VMEM((rows, cols), BF16),
            pltpu.VMEM((3, cols), F32),
            pltpu.VMEM((1, cols), F32),
            dma((6,)),
            dma((6 * z_n,)), dma((6 * z_n,)), dma((z_n,)), dma((z_n,)), dma((2,)),
            dma((3,)), dma((tp_n,)), dma((z_n,)), dma((z_n,)),
            dma((4 * z_n,)), dma((4 * z_n,)), dma((2,)),
            dma((fs_n,)), dma((fs_n,)), dma((fs_n,)), dma((fs_n,)),
            dma((2,)), dma((2,)),
        ],
        compiler_params=pltpu.CompilerParams(
            collective_id=0, has_side_effects=True, vmem_limit_bytes=56000 * 1024
        ),
    )(*args)


def per_device(fs_n, tp_n, up_pre, gate_value, out_cotangent, down_weight, conv_weight, conv_bias):
    rows, cols = up_pre.shape
    dblk = down_weight.shape[0]
    width = dblk * fs_n
    y_n = max(tp_n // 2, 2)
    z_n = fs_n // y_n
    args = tuple(
        pltpu.with_memory_space_constraint(value, pltpu.HBM)
        for value in (up_pre, gate_value, out_cotangent, down_weight, conv_weight, conv_bias[None, :])
    )
    if tp_n == 4 and z_n == tp_n and rows % 64 == 0 and cols % 256 == 0 and dblk % 128 == 0:
        outs = line_call(fs_n, tp_n, y_n, args)
    else:
        outs = general_call(fs_n, tp_n, y_n, args)
    ug, gg, wg, tap, bias, norm = outs
    return ug, gg, wg, tap, bias[0], norm[0]


def solution(mesh):
    return jax.shard_map(
        functools.partial(per_device, mesh.shape["fs"], mesh.shape["tp"]),
        mesh=mesh,
        in_specs=(
            P("fs", "tp"),
            P("fs", "tp"),
            P("fs", "tp"),
            P("fs", "tp"),
            P(None, "tp"),
            P("tp"),
        ),
        out_specs=(P("fs", "tp"), P("fs", "tp"), P("fs", "tp"), P(None, "tp"), P("tp"), P("tp")),
        check_vma=False,
    )
```

```python
import functools

import jax
import jax.numpy as jnp
from jax import lax
from jax.experimental import pallas as pl
from jax.experimental.pallas import tpu as pltpu
from jax.sharding import PartitionSpec as P

MESH = pl.DeviceIdType.MESH
F32 = jnp.float32
BF16 = jnp.bfloat16


def kernel(
    fs_n, tp_n, y_n,
    up_hbm, gate_hbm, cot_ref, w_ref, cw_hbm, cb_hbm,
    ug_ref, gg_ref, wg_ref, tap_ref, bias_ref, norm_ref,
    wfull, cotf, lhs_t, hidden, act, gfac, upf, cg, pf32, pbf,
    r1, s2, r2, st, nb, halo_up, halo_cg, up_ref, gate_ref, cw_ref, cb_ref,
    local_sem, w_recv, w_send_z, w_send_y, c_recv, c_send_x, c_send_m,
    r1_recv, r1_send, r2_recv, r2_send, st_recv, st_send, nb_recv, nb_send,
    hu_sem, hc_sem,
):
    rows, cols = up_hbm.shape
    dblk = w_ref.shape[0]
    cshard = cot_ref.shape[1]
    z_n = fs_n // y_n
    x_n = tp_n // 2
    me, tp = lax.axis_index("fs"), lax.axis_index("tp")
    mz, my = me // y_n, me % y_n
    mx, mc = tp // 2, tp % 2
    mate = mx * 2 + (1 - mc)
    sends = []

    def rcopy(src, dst, ss, rs, fs_id, tp_id):
        return pltpu.make_async_remote_copy(
            src_ref=src, dst_ref=dst, send_sem=ss, recv_sem=rs,
            device_id=(fs_id, tp_id), device_id_type=MESH,
        )

    def send(*args):
        copy = rcopy(*args)
        copy.start()
        sends.append(copy)

    def wrows(owner):
        return wfull.at[pl.ds(pl.multiple_of(owner * dblk, dblk), dblk)]

    def ccols(owner):
        return cotf.at[:, pl.ds(pl.multiple_of(owner * cshard, cshard), cshard)]

    own_w = pltpu.make_async_copy(w_ref, wrows(me), local_sem.at[0])
    own_c = pltpu.make_async_copy(cot_ref, ccols(tp), local_sem.at[1])
    loads = [
        pltpu.make_async_copy(src, dst, local_sem.at[k])
        for k, (src, dst) in enumerate(
            [(up_hbm, up_ref), (gate_hbm, gate_ref), (cw_hbm, cw_ref), (cb_hbm, cb_ref)], 2
        )
    ]

    barrier = pltpu.get_barrier_semaphore()
    peers = [((me + d) % fs_n, tp) for d in range(1, fs_n)]
    peers += [(me, ((mx + d) % x_n) * 2 + mc) for d in range(1, x_n)] + [(me, mate)]
    for peer in peers:
        pl.semaphore_signal(barrier, inc=1, device_id=peer, device_id_type=MESH)
    for copy in loads:
        copy.start()
    pl.semaphore_wait(barrier, len(peers))

    @pl.when(me < fs_n - 1)
    def _():
        rcopy(up_hbm.at[pl.ds(rows - 16, 16)], halo_up, hu_sem.at[0], hu_sem.at[1], me + 1, tp).start()

    for d in range(1, x_n):
        send(cot_ref, ccols(tp), c_send_x.at[d], c_recv.at[tp], me, ((mx + d) % x_n) * 2 + mc)
    for d in range(1, z_n):
        send(w_ref, wrows(me), w_send_z.at[d], w_recv.at[me], ((mz + d) % z_n) * y_n + my, tp)
    for d in range(1, y_n):
        send(w_ref, wrows(me), w_send_y.at[d], w_recv.at[me], mz * y_n + (my + d) % y_n, tp)
    send(cot_ref, ccols(tp), c_send_m.at[0], c_recv.at[tp], me, mate)
    own_w.start()
    own_c.start()

    for copy in loads:
        copy.wait()

    @pl.when(me > 0)
    def _():
        rcopy(halo_up, halo_up, hu_sem.at[0], hu_sem.at[1], me - 1, tp).wait_recv()
        upf[0:8] = halo_up[...].astype(F32)[8:16]

    @pl.when(me == 0)
    def _():
        upf[0:8] = jnp.zeros((8, cols), F32)

    upf[8 : rows + 8] = up_ref[...].astype(F32)
    step = 64

    @pl.loop(0, cols // 128)
    def _(j):
        lanes = pl.ds(pl.multiple_of(j * 128, 128), 128)
        taps = [cw_ref[k : k + 1, lanes] for k in range(3)]
        bias = cb_ref[0:1, lanes]
        for r in range(0, rows, step):
            conv = bias + taps[0] * upf[r + 6 : r + 6 + step, lanes]
            conv = conv + taps[1] * upf[r + 7 : r + 7 + step, lanes]
            conv = conv + taps[2] * upf[r + 8 : r + 8 + step, lanes]
            sig = 1.0 / (1.0 + jnp.exp(-conv))
            a = conv * sig
            g = gate_ref[r : r + step, lanes].astype(F32)
            act[r : r + step, lanes] = a
            hidden[r : r + step, lanes] = (a * g).astype(BF16)
            gfac[r : r + step, lanes] = g * sig * (1.0 + conv * (1.0 - sig))

    def wait_cot(d, other):
        owner = ((mx + x_n - d) % x_n) * 2 + (1 - mc if other else mc)
        sem = c_send_m if other else c_send_x
        rcopy(cot_ref, ccols(owner), sem.at[d], c_recv.at[owner], me, mate if other else owner).wait_recv()
        return owner

    ywide = y_n * dblk
    tile = min(256, cols)
    own_chunks = max(z_n // x_n, 1)

    def chunk(o):
        return (mx * own_chunks + o) % z_n

    def partial_grad(o):
        zp = chunk(o)
        base = pl.multiple_of(zp * ywide, ywide)
        lhs_t[...] = cotf[:, pl.ds(base, ywide)].T

        @pl.loop(0, cols // tile)
        def _(j):
            lanes = pl.ds(pl.multiple_of(j * tile, tile), tile)
            out = jnp.dot(lhs_t[...], hidden[:, lanes], preferred_element_type=F32)
            pf32[pl.ds(base, ywide), lanes] = out
            pbf[pl.ds(base, ywide), lanes] = out.astype(BF16)

        for e in range(1, y_n):
            yp = (my + e) % y_n
            block = pl.ds(pl.multiple_of((zp * y_n + yp) * dblk, dblk), dblk)
            sem = (e - 1) * z_n + o
            send(pbf.at[block], r1.at[e - 1, o], r1_send.at[sem], r1_recv.at[sem], mz * y_n + yp, tp)

    own_c.wait()
    wait_cot(0, True)
    for o in range(own_chunks):
        partial_grad(o)
    for d in range(1, x_n):
        owner = wait_cot(d, False)
        send(ccols(owner), ccols(owner), c_send_m.at[d], c_recv.at[owner], me, mate)
    for d in range(1, x_n):
        wait_cot(d, True)
    for o in range(own_chunks, z_n):
        partial_grad(o)

    def y_sum_wait(o):
        for e in range(1, y_n):
            sem = (e - 1) * z_n + o
            rcopy(r1.at[e - 1, o], r1.at[e - 1, o], r1_send.at[sem], r1_recv.at[sem],
                  mz * y_n + (my + e) % y_n, tp).wait_recv()

    def y_sum(o, block, lanes):
        total = pf32[block, lanes]
        for e in range(1, y_n):
            total = total + r1[e - 1, o, :, lanes].astype(F32)
        return total

    def z_copy(o):
        return rcopy(s2.at[o], r2.at[mz], r2_send.at[o], r2_recv.at[mz], chunk(o) * y_n + my, tp)

    def sum_and_send(o):
        zp = chunk(o)
        block = pl.ds(pl.multiple_of((zp * y_n + my) * dblk, dblk), dblk)
        y_sum_wait(o)

        @pl.when(zp != mz)
        def _():
            @pl.loop(0, cols // 128)
            def _(j):
                lanes = pl.ds(pl.multiple_of(j * 128, 128), 128)
                s2[o, :, lanes] = y_sum(o, block, lanes).astype(BF16)

            z_copy(o).start()

    early = z_n // 2
    for o in range(early):
        sum_and_send(o)

    own_w.wait()
    for d in range(1, z_n):
        owner = ((mz + z_n - d) % z_n) * y_n + my
        rcopy(w_ref, wrows(owner), w_send_z.at[d], w_recv.at[owner], owner, tp).wait_recv()
        for e in range(1, y_n):
            send(wrows(owner), wrows(owner), w_send_y.at[d * y_n + e], w_recv.at[owner],
                 mz * y_n + (my + e) % y_n, tp)

    part_rows = 256

    def add_block(owner, first, last):
        wide = pl.multiple_of(owner * dblk, dblk)

        @pl.loop(0, cols // tile)
        def _(j):
            lanes = pl.ds(pl.multiple_of(j * tile, tile), tile)

            @pl.loop(0, rows // part_rows)
            def _(i):
                part = pl.ds(pl.multiple_of(i * part_rows, part_rows), part_rows)
                hg = jnp.dot(cotf[part, pl.ds(wide, dblk)], wfull[pl.ds(wide, dblk), lanes], preferred_element_type=F32)
                if not first:
                    hg = hg + cg[part, lanes]
                if last:
                    gg_ref[part, lanes] = (hg * act[part, lanes]).astype(BF16)
                    hg = hg * gfac[part, lanes]
                cg[part, lanes] = hg

    sum_and_send(early)
    small = dblk % 128 != 0
    if not small:
        for d in range(z_n):
            add_block(((mz + z_n - d) % z_n) * y_n + my, d == 0, False)
    for o in range(early + 1, z_n):
        sum_and_send(o)
    for d in range(z_n):
        for e in range(1, y_n):
            owner = ((mz + z_n - d) % z_n) * y_n + (my + y_n - e) % y_n
            rcopy(wrows(owner), wrows(owner), w_send_y.at[d * y_n + e], w_recv.at[owner],
                  mz * y_n + (my + e) % y_n, tp).wait_recv()
            if not small:
                add_block(owner, False, d == z_n - 1 and e == y_n - 1)
    if small:

        @pl.loop(0, cols // tile)
        def _(j):
            lanes = pl.ds(pl.multiple_of(j * tile, tile), tile)

            @pl.loop(0, rows // part_rows)
            def _(i):
                part = pl.ds(pl.multiple_of(i * part_rows, part_rows), part_rows)
                hg = jnp.dot(cotf[part, :], wfull[:, lanes], preferred_element_type=F32)
                gg_ref[part, lanes] = (hg * act[part, lanes]).astype(BF16)
                cg[part, lanes] = hg * gfac[part, lanes]

    @pl.when(me > 0)
    def _():
        rcopy(cg.at[pl.ds(0, 8)], halo_cg, hc_sem.at[0], hc_sem.at[1], me - 1, tp).start()

    @pl.loop(0, cols // 128)
    def _(j):
        lanes = pl.ds(pl.multiple_of(j * 128, 128), 128)
        sums = [jnp.zeros((8, 128), F32) for _ in range(4)]
        for r in range(0, rows, step):
            grad = cg[r : r + step, lanes]
            terms = [grad * upf[r + 6 + k : r + 6 + k + step, lanes] for k in range(3)] + [grad]
            sums = [s + jnp.sum(t.reshape(step // 8, 8, 128), axis=0) for s, t in zip(sums, terms)]
        for k in range(4):
            st[me, k : k + 1, lanes] = jnp.sum(sums[k], axis=0, keepdims=True)
        st[me, 4:8, lanes] = jnp.zeros((4, 128), F32)

    for d in range(1, fs_n):
        send(st.at[me], st.at[me], st_send.at[d], st_recv.at[me], (me + d) % fs_n, tp)

    mine = (mz + z_n - chunk(0)) % z_n
    for d in range(1, z_n):
        zp = (mz + d) % z_n
        rcopy(s2.at[0], r2.at[zp], r2_send.at[0], r2_recv.at[zp], zp * y_n + my, tp).wait_recv()
    own_block = pl.ds(pl.multiple_of(me * dblk, dblk), dblk)

    @pl.loop(0, cols // 128)
    def _(j):
        lanes = pl.ds(pl.multiple_of(j * 128, 128), 128)
        total = y_sum(mine, own_block, lanes)
        for d in range(1, z_n):
            total = total + r2[(mz + d) % z_n, :, lanes].astype(F32)
        wg_ref[:, lanes] = total
        nb[me, :, lanes] = jnp.sum(total * total, axis=0, keepdims=True)

    for d in range(1, fs_n):
        send(nb.at[me], nb.at[me], nb_send.at[d], nb_recv.at[me], (me + d) % fs_n, tp)

    @pl.when(me < fs_n - 1)
    def _():
        rcopy(halo_cg, halo_cg, hc_sem.at[0], hc_sem.at[1], me + 1, tp).wait_recv()
        cg[rows : rows + 8] = halo_cg[...]

    @pl.when(me == fs_n - 1)
    def _():
        cg[rows : rows + 8] = jnp.zeros((8, cols), F32)

    @pl.loop(0, cols // 128)
    def _(j):
        lanes = pl.ds(pl.multiple_of(j * 128, 128), 128)
        taps = [cw_ref[k : k + 1, lanes] for k in range(3)]
        for r in range(0, rows, step):
            total = taps[0] * cg[r + 2 : r + 2 + step, lanes]
            total = total + taps[1] * cg[r + 1 : r + 1 + step, lanes]
            total = total + taps[2] * cg[r : r + step, lanes]
            ug_ref[r : r + step, lanes] = total.astype(BF16)

    for d in range(1, fs_n):
        owner = (me + d) % fs_n
        rcopy(st.at[owner], st.at[owner], st_send.at[d], st_recv.at[owner], owner, tp).wait_recv()
    stats = st[0]
    for k in range(1, fs_n):
        stats = stats + st[k]
    tap_ref[...] = stats[0:3]
    bias_ref[...] = stats[3:4]
    for d in range(1, fs_n):
        owner = (me + d) % fs_n
        rcopy(nb.at[owner], nb.at[owner], nb_send.at[d], nb_recv.at[owner], owner, tp).wait_recv()
    norms = nb[0]
    for k in range(1, fs_n):
        norms = norms + nb[k]
    norm_ref[...] = norms

    for copy in sends:
        copy.wait_send()
    for o in range(z_n):

        @pl.when(chunk(o) != mz)
        def _():
            z_copy(o).wait_send()

    @pl.when(me < fs_n - 1)
    def _():
        rcopy(up_hbm.at[pl.ds(rows - 16, 16)], halo_up, hu_sem.at[0], hu_sem.at[1], me + 1, tp).wait_send()

    @pl.when(me > 0)
    def _():
        rcopy(cg.at[pl.ds(0, 8)], halo_cg, hc_sem.at[0], hc_sem.at[1], me - 1, tp).wait_send()


def general_call(fs_n, tp_n, y_n, args):
    up_pre, _, _, down_weight, _, _ = args
    rows, cols = up_pre.shape
    dblk = down_weight.shape[0]
    width = dblk * fs_n
    z_n = fs_n // y_n
    dma = pltpu.SemaphoreType.DMA
    vmem = pl.BlockSpec(memory_space=pltpu.VMEM)
    return pl.pallas_call(
        functools.partial(kernel, fs_n, tp_n, y_n),
        out_shape=(
            jax.ShapeDtypeStruct((rows, cols), BF16),
            jax.ShapeDtypeStruct((rows, cols), BF16),
            jax.ShapeDtypeStruct((dblk, cols), F32),
            jax.ShapeDtypeStruct((3, cols), F32),
            jax.ShapeDtypeStruct((1, cols), F32),
            jax.ShapeDtypeStruct((1, cols), F32),
        ),
        in_specs=[pl.BlockSpec(memory_space=pltpu.HBM)] * 6,
        out_specs=[vmem] * 6,
        scratch_shapes=[
            pltpu.VMEM((width, cols), BF16),
            pltpu.VMEM((rows, width), BF16),
            pltpu.VMEM((y_n * dblk, rows), BF16),
            pltpu.VMEM((rows, cols), BF16),
            pltpu.VMEM((rows, cols), F32),
            pltpu.VMEM((rows, cols), F32),
            pltpu.VMEM((rows + 8, cols), F32),
            pltpu.VMEM((rows + 8, cols), F32),
            pltpu.VMEM((width, cols), F32),
            pltpu.VMEM((width, cols), BF16),
            pltpu.VMEM((y_n - 1, z_n, dblk, cols), BF16),
            pltpu.VMEM((z_n, dblk, cols), BF16),
            pltpu.VMEM((z_n, dblk, cols), BF16),
            pltpu.VMEM((fs_n, 8, cols), F32),
            pltpu.VMEM((fs_n, 1, cols), F32),
            pltpu.VMEM((16, cols), BF16),
            pltpu.VMEM((8, cols), F32),
            pltpu.VMEM((rows, cols), BF16),
            pltpu.VMEM((rows, cols), BF16),
            pltpu.VMEM((3, cols), F32),
            pltpu.VMEM((1, cols), F32),
            dma((6,)),
            dma((fs_n,)), dma((z_n,)), dma((z_n * y_n,)),
            dma((tp_n,)), dma((tp_n // 2,)), dma((tp_n // 2,)),
            dma(((y_n - 1) * z_n,)), dma(((y_n - 1) * z_n,)),
            dma((z_n,)), dma((z_n,)),
            dma((fs_n,)), dma((fs_n,)), dma((fs_n,)), dma((fs_n,)),
            dma((2,)), dma((2,)),
        ],
        compiler_params=pltpu.CompilerParams(
            collective_id=0, has_side_effects=True, vmem_limit_bytes=48000 * 1024
        ),
    )(*args)


def line_kernel(
    fs_n, tp_n, y_n, n1,
    up_hbm, gate_hbm, cot_hbm, w_hbm, cw_hbm, cb_hbm,
    ug_ref, gg_ref, wg_ref, tap_ref, bias_ref, norm_ref,
    wfull, cotf, lhs_t, hidden, act, gfac, upf, cg, pf32,
    ysend, yrecv, sz1, rz1, sz2, rz2, sf, rf,
    sy, st, nb, halo_up, halo_cg, cw_ref, cb_ref,
    local_sem, ag_send, ag_recv, yw_send, yw_recv, yp_sem, c_send, c_recv, ry_send, ry_recv,
    rs_send, rs_recv, f_sem, st_recv, st_send, nb_recv, nb_send, hu_sem, hc_sem,
):
    rows, cols = up_hbm.shape
    dblk = w_hbm.shape[0]
    cshard = cot_hbm.shape[1]
    ywide = y_n * dblk
    z_n = fs_n // y_n
    n2 = cols - n1
    me, tp = lax.axis_index("fs"), lax.axis_index("tp")
    mz, my = me // y_n, me % y_n
    mx, mc = tp // 2, tp % 2
    mate = mx * 2 + (1 - mc)
    mirror = (1 - mx) * 2 + mc
    ynb = mz * y_n + (1 - my)
    sign = (1, -1)
    avail = (mz, z_n - 1 - mz)
    has_next = (mz < z_n - 1, mz > 0)
    has_prev = (mz > 0, mz < z_n - 1)
    nxt = [((mz + z_n + s) % z_n) * y_n + my for s in sign]
    sends = []

    def rcopy(src, dst, ss, rs, fs_id, tp_id):
        return pltpu.make_async_remote_copy(
            src_ref=src, dst_ref=dst, send_sem=ss, recv_sem=rs,
            device_id=(fs_id, tp_id), device_id_type=MESH,
        )

    def start(make, pred=None, inside=None):
        if pred is None:
            make().start()
        else:
            @pl.when(pred if inside is None else inside)
            def _():
                make().start()
        sends.append((pred, make))

    def drows(zp, y):
        return pl.ds(pl.multiple_of((zp * y_n + y) * dblk, dblk), dblk)

    half_rows = rows // 2

    def ccols(owner):
        return cotf.at[:, pl.ds(pl.multiple_of(owner * cshard, cshard), cshard)]

    def chalf(owner, half):
        tokens = pl.ds(pl.multiple_of(half * half_rows, half_rows), half_rows)
        return cotf.at[tokens, pl.ds(pl.multiple_of(owner * cshard, cshard), cshard)]

    def urgent(side):
        outer = side * (z_n - 1)
        return jnp.where(mz == outer, side * (z_n // 2) + 1 - side, outer)

    def other(side, quarter):
        return 2 * side * (z_n // 2) + 1 - quarter

    def cx_copy(order, src=None):
        quarter = urgent(mx) if order == 0 else other(mx, urgent(mx))
        ref = chalf(quarter, mc)
        return rcopy(ref if src is None else src, ref, c_send.at[order], c_recv.at[order], me, mirror)

    def cm_copy(order, half):
        quarter = urgent(1 - mx) if order == 0 else other(1 - mx, urgent(1 - mx))
        ref = chalf(quarter, half)
        return rcopy(ref, ref, c_send.at[2 + order], c_recv.at[2 + order], me, mate)

    part1, part2 = pl.ds(0, n1), pl.ds(n1, n2)

    def ag_copy(d, slot, part, zp):
        ref = wfull.at[drows(zp, 1 - my if part == 2 else my), part1 if part == 1 else part2]
        src = ref
        if slot == 0 and part < 2:
            src = w_hbm.at[:, part1 if part == 1 else part2]
        i = (d * z_n + slot) * 3 + part
        return rcopy(src, ref, ag_send.at[i], ag_recv.at[i], nxt[d], tp)

    def yw_copy(zp, own=False):
        ref = wfull.at[drows(zp, my), part1]
        return rcopy(w_hbm.at[:, part1] if own else ref, ref, yw_send.at[zp], yw_recv.at[zp], ynb, tp)

    def yw_wait(zp):
        ref = wfull.at[drows(zp, 1 - my), part1]
        rcopy(ref, ref, yw_send.at[zp], yw_recv.at[zp], ynb, tp).wait_recv()

    def rs_copy(d, slot, part, t):
        i = (d * z_n + slot) * 2 + part
        slot_to = z_n if d == 1 and slot == z_n - 1 else t
        src, dst = (sz2.at[t], rz2.at[slot_to]) if part == 0 else (sz1.at[t], rz1.at[slot_to])
        return rcopy(src, dst, rs_send.at[i], rs_recv.at[i], nxt[d], tp)

    def ry_copy(t):
        return rcopy(ysend.at[t], yrecv.at[t], ry_send.at[t], ry_recv.at[t], ynb, tp)

    own_w = pltpu.make_async_copy(w_hbm, wfull.at[drows(mz, my)], local_sem.at[0])
    own_c = pltpu.make_async_copy(cot_hbm, ccols(tp), local_sem.at[1])
    loads = [
        pltpu.make_async_copy(src, dst, local_sem.at[k])
        for k, (src, dst) in enumerate(
            [(up_hbm, ug_ref), (gate_hbm, gg_ref), (cw_hbm, cw_ref), (cb_hbm, cb_ref)], 2
        )
    ]

    barrier = pltpu.get_barrier_semaphore()
    peers = [((me + d) % fs_n, tp) for d in range(1, fs_n)] + [(me, mirror), (me, mate)]
    for peer in peers:
        pl.semaphore_signal(barrier, inc=1, device_id=peer, device_id_type=MESH)
    for copy in loads:
        copy.start()
    own_c.start()
    own_w.start()
    pl.semaphore_wait(barrier, len(peers))

    start(
        lambda: rcopy(up_hbm.at[pl.ds(rows - 16, 16)], halo_up, hu_sem.at[0], hu_sem.at[1], (me + 1) % fs_n, tp),
        me < fs_n - 1,
    )
    yp_copy = lambda: rcopy(
        w_hbm.at[:, part2], wfull.at[drows(mz, my), part2], yp_sem.at[0], yp_sem.at[1], ynb, tp
    )
    start(yp_copy)
    for part in (0, 1):
        for d in (0, 1):
            start(functools.partial(ag_copy, d, 0, part, mz), has_next[d])
    start(functools.partial(yw_copy, mz, True))
    start(lambda: rcopy(cot_hbm, ccols(tp), c_send.at[4], c_recv.at[4], me, mate))
    own_half = cot_hbm.at[pl.ds(pl.multiple_of(mc * half_rows, half_rows), half_rows)]
    leads = urgent(mx) == tp

    @pl.when(leads)
    def _():
        cx_copy(0, own_half).start()

    for copy in loads:
        copy.wait()

    @pl.when(me > 0)
    def _():
        rcopy(halo_up, halo_up, hu_sem.at[0], hu_sem.at[1], (me + fs_n - 1) % fs_n, tp).wait_recv()
        upf[0:8] = halo_up[...].astype(F32)[8:16]

    @pl.when(me == 0)
    def _():
        upf[0:8] = jnp.zeros((8, cols), F32)

    rcopy(cot_hbm, ccols(mate), c_send.at[4], c_recv.at[4], me, mate).wait_recv()

    @pl.when(leads)
    def _():
        cx_copy(1).start()

    @pl.when(jnp.logical_not(leads))
    def _():
        cx_copy(0).start()
        cx_copy(1, own_half).start()

    sends.append((None, functools.partial(cx_copy, 0)))
    sends.append((None, functools.partial(cx_copy, 1)))

    upf[8 : rows + 8] = ug_ref[...].astype(F32)
    step = 64

    @pl.loop(0, cols // 128)
    def _(j):
        lanes = pl.ds(pl.multiple_of(j * 128, 128), 128)
        taps = [cw_ref[k : k + 1, lanes] for k in range(3)]
        bias = cb_ref[0:1, lanes]
        for r in range(0, rows, step):
            conv = bias + taps[0] * upf[r + 6 : r + 6 + step, lanes]
            conv = conv + taps[1] * upf[r + 7 : r + 7 + step, lanes]
            conv = conv + taps[2] * upf[r + 8 : r + 8 + step, lanes]
            sig = 1.0 / (1.0 + jnp.exp(-conv))
            a = conv * sig
            g = gg_ref[r : r + step, lanes].astype(F32)
            act[r : r + step, lanes] = a
            hidden[r : r + step, lanes] = (a * g).astype(BF16)
            gfac[r : r + step, lanes] = g * sig * (1.0 + conv * (1.0 - sig))

    rcopy(
        w_hbm.at[:, part2], wfull.at[drows(mz, 1 - my), part2], yp_sem.at[0], yp_sem.at[1], ynb, tp
    ).wait_recv()
    for d in (0, 1):
        start(functools.partial(ag_copy, d, 0, 2, mz), has_next[d])

    tile = min(256, cols)

    def wg_part(t):
        base = pl.multiple_of(t * ywide, ywide)
        lhs_t[...] = cotf[:, pl.ds(base, ywide)].T

        @pl.loop(0, cols // tile)
        def _(j):
            lanes = pl.ds(pl.multiple_of(j * tile, tile), tile)
            pf32[pl.ds(base, ywide), lanes] = jnp.dot(lhs_t[...], hidden[:, lanes], preferred_element_type=F32)

        @pl.loop(0, n1 // 128)
        def _(j):
            lanes = pl.ds(pl.multiple_of(j * 128, 128), 128)
            ysend[t, :, lanes] = pf32[drows(t, 1 - my), lanes].astype(BF16)

    def ry_start(delta, only=None):
        for s in sign if delta else (1,):
            t = mz + s * delta
            pred = (t >= 0) & (t < z_n)
            t = (t + z_n) % z_n
            if only is not None:
                pred = pred & (t == only)
            start(functools.partial(ry_copy, t), pred)

    def wg_far(order):
        cx = urgent(1 - mx) if order == 0 else other(1 - mx, urgent(1 - mx))
        rcopy(chalf(cx, mc), chalf(cx, mc), c_send.at[order], c_recv.at[order], me, mirror).wait_recv()
        start(functools.partial(cm_copy, order, mc))
        cm_copy(order, 1 - mc).wait_recv()
        wg_part(cx)

    own_c.wait()
    wg_part(urgent(mx))
    ry_start(z_n - 1, urgent(mx))
    wg_far(0)
    ry_start(z_n - 1, urgent(1 - mx))
    wg_part(other(mx, urgent(mx)))
    def ag_step(k):
        for d in (0, 1):
            zp = (mz + z_n - sign[d] * (1 + k)) % z_n
            is_ag = k < avail[d]
            fwd = is_ag & has_next[d]

            @pl.when(is_ag)
            def _():
                for part in (0, 1, 2):
                    ag_copy(d, k, part, zp).wait_recv()
                    if k + 1 < z_n - 1:
                        @pl.when(has_next[d])
                        def _():
                            ag_copy(d, k + 1, part, zp).start()
                    if part == 1:
                        yw_copy(zp).start()

            for part in (0, 1, 2):
                if k + 1 < z_n - 1:
                    sends.append((fwd, functools.partial(ag_copy, d, k + 1, part, zp)))
            sends.append((is_ag, functools.partial(yw_copy, zp)))

    def rs_step(k, part):
        for d in (0, 1):
            t = (mz + z_n - sign[d] * (1 + k)) % z_n
            pred = k >= avail[d]

            def run(arrived, d=d, t=t):
                if part == 1:
                    ry_copy(t).wait_recv()
                if arrived:
                    rs_copy(d, k, part, t).wait_recv()

                @pl.loop(0, (n1 if part else n2) // 128)
                def _(j):
                    near = pl.ds(pl.multiple_of(j * 128, 128), 128)
                    if part == 1:
                        total = pf32[drows(t, my), near] + yrecv[t, :, near].astype(F32)
                    else:
                        far = pl.ds(pl.multiple_of(n1 + j * 128, 128), 128)
                        total = pf32[pl.ds(pl.multiple_of(t * ywide, ywide), ywide), far]
                    if arrived:
                        total = total + (rz1 if part else rz2)[t, :, near].astype(F32)
                    (sz1 if part else sz2)[t, :, near] = total.astype(BF16)

                rs_copy(d, k + 1, part, t).start()

            if k > 0:
                pl.when(pred & has_prev[d])(functools.partial(run, True))
            pl.when(pred & jnp.logical_not(has_prev[d]))(functools.partial(run, False))
            sends.append((pred, functools.partial(rs_copy, d, k + 1, part, t)))

    part_rows = rows // 2 if rows % 32 == 0 else rows

    def hg_add(zp, first):
        base = pl.ds(pl.multiple_of(zp * ywide, ywide), ywide)

        @pl.loop(0, cols // tile)
        def _(j):
            lanes = pl.ds(pl.multiple_of(j * tile, tile), tile)

            @pl.loop(0, rows // part_rows)
            def _(i):
                part = pl.ds(pl.multiple_of(i * part_rows, part_rows), part_rows)
                hg = jnp.dot(cotf[part, base], wfull[base, lanes], preferred_element_type=F32)
                if not first:
                    hg = hg + cg[part, lanes]
                cg[part, lanes] = hg

    def hg_far(delta):
        for s in sign:
            zp = mz + s * delta

            @pl.when((zp >= 0) & (zp < z_n))
            def _():
                near = (zp + z_n) % z_n
                yw_wait(near)
                hg_add(near, False)

    ag_step(0)
    rs_step(0, 0)
    wg_far(1)
    for delta in range(z_n - 2, 1, -1):
        ry_start(delta)
    own_w.wait()
    yw_wait(mz)
    hg_add(mz, True)
    rs_step(0, 1)
    ag_step(1)
    ry_start(1)
    rs_step(1, 0)
    rs_step(1, 1)
    hg_far(1)
    ag_step(2)
    ry_start(0)
    rs_step(2, 0)
    rs_step(2, 1)
    hg_far(2)
    hg_far(z_n - 1)

    @pl.loop(0, cols // 128)
    def _(j):
        lanes = pl.ds(pl.multiple_of(j * 128, 128), 128)
        for r in range(0, rows, step):
            part = slice(r, r + step)
            hg = cg[part, lanes]
            gg_ref[part, lanes] = (hg * act[part, lanes]).astype(BF16)
            cg[part, lanes] = hg * gfac[part, lanes]

    start(
        lambda: rcopy(cg.at[pl.ds(0, 8)], halo_cg, hc_sem.at[0], hc_sem.at[1], (me + fs_n - 1) % fs_n, tp),
        me > 0,
    )

    @pl.loop(0, cols // 128)
    def _(j):
        lanes = pl.ds(pl.multiple_of(j * 128, 128), 128)
        sums = [jnp.zeros((8, 128), F32) for _ in range(4)]
        for r in range(0, rows, step):
            grad = cg[r : r + step, lanes]
            terms = [grad * upf[r + 6 + k : r + 6 + k + step, lanes] for k in range(3)] + [grad]
            sums = [s + jnp.sum(t.reshape(step // 8, 8, 128), axis=0) for s, t in zip(sums, terms)]
        for k in range(4):
            sy[my, k : k + 1, lanes] = jnp.sum(sums[k], axis=0, keepdims=True)

    start(lambda: rcopy(sy.at[my], sy.at[my], st_send.at[0], st_recv.at[z_n], ynb, tp))

    last = z_n - 1
    for d in (0, 1):

        @pl.when(has_prev[d])
        def _():
            rs_copy(d, last, 0, mz).wait_recv()

            @pl.loop(0, n2 // 128)
            def _(j):
                far = pl.ds(pl.multiple_of(n1 + j * 128, 128), 128)
                near = pl.ds(pl.multiple_of(j * 128, 128), 128)
                block = pl.ds(pl.multiple_of(mz * ywide, ywide), ywide)
                pf32[block, far] = pf32[block, far] + rz2[z_n if d == 1 else mz, :, near].astype(F32)

    @pl.loop(0, n2 // 128)
    def _(j):
        far = pl.ds(pl.multiple_of(n1 + j * 128, 128), 128)
        near = pl.ds(pl.multiple_of(j * 128, 128), 128)
        sf[:, near] = pf32[drows(mz, 1 - my), far].astype(BF16)

    f_copy = lambda: rcopy(sf, rf, f_sem.at[0], f_sem.at[1], ynb, tp)
    start(f_copy)

    rcopy(sy.at[1 - my], sy.at[1 - my], st_send.at[0], st_recv.at[z_n], ynb, tp).wait_recv()
    st[mz] = sy[0] + sy[1]
    for d in range(1, z_n):
        start(
            lambda d=d: rcopy(
                st.at[mz], st.at[mz], st_send.at[d], st_recv.at[mz], ((mz + d) % z_n) * y_n + my, tp
            )
        )

    own_block = drows(mz, my)
    ry_copy(mz).wait_recv()

    @pl.loop(0, n1 // 128)
    def _(j):
        lanes = pl.ds(pl.multiple_of(j * 128, 128), 128)
        wg_ref[:, lanes] = pf32[own_block, lanes] + yrecv[mz, :, lanes].astype(F32)

    for d in (0, 1):

        @pl.when(has_prev[d])
        def _():
            rs_copy(d, last, 1, mz).wait_recv()

            @pl.loop(0, n1 // 128)
            def _(j):
                lanes = pl.ds(pl.multiple_of(j * 128, 128), 128)
                wg_ref[:, lanes] = wg_ref[:, lanes] + rz1[z_n if d == 1 else mz, :, lanes].astype(F32)

    f_copy().wait_recv()

    @pl.loop(0, n2 // 128)
    def _(j):
        far = pl.ds(pl.multiple_of(n1 + j * 128, 128), 128)
        near = pl.ds(pl.multiple_of(j * 128, 128), 128)
        wg_ref[:, far] = pf32[own_block, far] + rf[:, near].astype(F32)

    @pl.loop(0, cols // 128)
    def _(j):
        lanes = pl.ds(pl.multiple_of(j * 128, 128), 128)
        total = wg_ref[:, lanes]
        nb[me, :, lanes] = jnp.sum(total * total, axis=0, keepdims=True)

    for d in range(1, fs_n):
        start(
            lambda d=d: rcopy(nb.at[me], nb.at[me], nb_send.at[d], nb_recv.at[me], (me + d) % fs_n, tp)
        )

    @pl.when(me < fs_n - 1)
    def _():
        rcopy(halo_cg, halo_cg, hc_sem.at[0], hc_sem.at[1], (me + 1) % fs_n, tp).wait_recv()
        cg[rows : rows + 8] = halo_cg[...]

    @pl.when(me == fs_n - 1)
    def _():
        cg[rows : rows + 8] = jnp.zeros((8, cols), F32)

    @pl.loop(0, cols // 128)
    def _(j):
        lanes = pl.ds(pl.multiple_of(j * 128, 128), 128)
        taps = [cw_ref[k : k + 1, lanes] for k in range(3)]
        for r in range(0, rows, step):
            total = taps[0] * cg[r + 2 : r + 2 + step, lanes]
            total = total + taps[1] * cg[r + 1 : r + 1 + step, lanes]
            total = total + taps[2] * cg[r : r + step, lanes]
            ug_ref[r : r + step, lanes] = total.astype(BF16)

    for d in range(1, z_n):
        zp = (mz + d) % z_n
        rcopy(st.at[zp], st.at[zp], st_send.at[d], st_recv.at[zp], zp * y_n + my, tp).wait_recv()
    stats = st[0]
    for d in range(1, z_n):
        stats = stats + st[d]
    tap_ref[...] = stats[0:3]
    bias_ref[...] = stats[3:4]

    for pred, make in sends:
        if pred is None:
            make().wait_send()
        else:
            @pl.when(pred)
            def _():
                make().wait_send()

    for d in range(1, fs_n):
        owner = (me + d) % fs_n
        rcopy(nb.at[owner], nb.at[owner], nb_send.at[d], nb_recv.at[owner], owner, tp).wait_recv()
    norms = nb[0]
    for k in range(1, fs_n):
        norms = norms + nb[k]
    norm_ref[...] = norms


def line_call(fs_n, tp_n, y_n, args):
    up_pre, _, _, down_weight, _, _ = args
    rows, cols = up_pre.shape
    dblk = down_weight.shape[0]
    width = dblk * fs_n
    ywide = y_n * dblk
    z_n = fs_n // y_n
    n2 = max(cols * 3 // 8 // 128, 1) * 128
    n1 = cols - n2
    dma = pltpu.SemaphoreType.DMA
    vmem = pl.BlockSpec(memory_space=pltpu.VMEM)
    return pl.pallas_call(
        functools.partial(line_kernel, fs_n, tp_n, y_n, n1),
        out_shape=(
            jax.ShapeDtypeStruct((rows, cols), BF16),
            jax.ShapeDtypeStruct((rows, cols), BF16),
            jax.ShapeDtypeStruct((dblk, cols), F32),
            jax.ShapeDtypeStruct((3, cols), F32),
            jax.ShapeDtypeStruct((1, cols), F32),
            jax.ShapeDtypeStruct((1, cols), F32),
        ),
        in_specs=[pl.BlockSpec(memory_space=pltpu.HBM)] * 6,
        out_specs=[vmem] * 6,
        scratch_shapes=[
            pltpu.VMEM((width, cols), BF16),
            pltpu.VMEM((rows, width), BF16),
            pltpu.VMEM((ywide, rows), BF16),
            pltpu.VMEM((rows, cols), BF16),
            pltpu.VMEM((rows, cols), F32),
            pltpu.VMEM((rows, cols), F32),
            pltpu.VMEM((rows + 8, cols), F32),
            pltpu.VMEM((rows + 8, cols), F32),
            pltpu.VMEM((width, cols), F32),
            pltpu.VMEM((z_n, dblk, n1), BF16),
            pltpu.VMEM((z_n, dblk, n1), BF16),
            pltpu.VMEM((z_n, dblk, n1), BF16),
            pltpu.VMEM((z_n + 1, dblk, n1), BF16),
            pltpu.VMEM((z_n, ywide, n2), BF16),
            pltpu.VMEM((z_n + 1, ywide, n2), BF16),
            pltpu.VMEM((dblk, n2), BF16),
            pltpu.VMEM((dblk, n2), BF16),
            pltpu.VMEM((y_n, 4, cols), F32),
            pltpu.VMEM((z_n, 4, cols), F32),
            pltpu.VMEM((fs_n, 1, cols), F32),
            pltpu.VMEM((16, cols), BF16),
            pltpu.VMEM((8, cols), F32),
            pltpu.VMEM((3, cols), F32),
            pltpu.VMEM((1, cols), F32),
            dma((6,)),
            dma((6 * z_n,)), dma((6 * z_n,)), dma((z_n,)), dma((z_n,)), dma((2,)),
            dma((5,)), dma((5,)), dma((z_n,)), dma((z_n,)),
            dma((4 * z_n,)), dma((4 * z_n,)), dma((2,)),
            dma((fs_n,)), dma((z_n,)), dma((fs_n,)), dma((fs_n,)),
            dma((2,)), dma((2,)),
        ],
        compiler_params=pltpu.CompilerParams(
            collective_id=0, has_side_effects=True, vmem_limit_bytes=46000 * 1024
        ),
    )(*args)


def per_device(fs_n, tp_n, up_pre, gate_value, out_cotangent, down_weight, conv_weight, conv_bias):
    rows, cols = up_pre.shape
    dblk = down_weight.shape[0]
    width = dblk * fs_n
    y_n = max(tp_n // 2, 2)
    z_n = fs_n // y_n
    args = tuple(
        pltpu.with_memory_space_constraint(value, pltpu.HBM)
        for value in (up_pre, gate_value, out_cotangent, down_weight, conv_weight, conv_bias[None, :])
    )
    if tp_n == 4 and z_n == tp_n and rows % 64 == 0 and cols % 256 == 0 and dblk % 128 == 0:
        outs = line_call(fs_n, tp_n, y_n, args)
    else:
        outs = general_call(fs_n, tp_n, y_n, args)
    ug, gg, wg, tap, bias, norm = outs
    return ug, gg, wg, tap, bias[0], norm[0]


def solution(mesh):
    return jax.shard_map(
        functools.partial(per_device, mesh.shape["fs"], mesh.shape["tp"]),
        mesh=mesh,
        in_specs=(
            P("fs", "tp"),
            P("fs", "tp"),
            P("fs", "tp"),
            P("fs", "tp"),
            P(None, "tp"),
            P("tp"),
        ),
        out_specs=(P("fs", "tp"), P("fs", "tp"), P("fs", "tp"), P(None, "tp"), P("tp"), P("tp")),
        check_vma=False,
    )
```

```python
import functools

import jax
import jax.numpy as jnp
from jax import lax
from jax.experimental import pallas as pl
from jax.experimental.pallas import tpu as pltpu
from jax.sharding import PartitionSpec as P

MESH = pl.DeviceIdType.MESH
F32 = jnp.float32
BF16 = jnp.bfloat16


def kernel(
    fs_n, tp_n, y_n,
    up_hbm, gate_hbm, cot_ref, w_ref, cw_hbm, cb_hbm,
    ug_ref, gg_ref, wg_ref, tap_ref, bias_ref, norm_ref,
    wfull, cotf, lhs_t, hidden, act, gfac, upf, cg, pf32, pbf,
    r1, s2, r2, st, nb, halo_up, halo_cg, up_ref, gate_ref, cw_ref, cb_ref,
    local_sem, w_recv, w_send_z, w_send_y, c_recv, c_send_x, c_send_m,
    r1_recv, r1_send, r2_recv, r2_send, st_recv, st_send, nb_recv, nb_send,
    hu_sem, hc_sem,
):
    rows, cols = up_hbm.shape
    dblk = w_ref.shape[0]
    cshard = cot_ref.shape[1]
    z_n = fs_n // y_n
    x_n = tp_n // 2
    me, tp = lax.axis_index("fs"), lax.axis_index("tp")
    mz, my = me // y_n, me % y_n
    mx, mc = tp // 2, tp % 2
    mate = mx * 2 + (1 - mc)
    sends = []

    def rcopy(src, dst, ss, rs, fs_id, tp_id):
        return pltpu.make_async_remote_copy(
            src_ref=src, dst_ref=dst, send_sem=ss, recv_sem=rs,
            device_id=(fs_id, tp_id), device_id_type=MESH,
        )

    def send(*args):
        copy = rcopy(*args)
        copy.start()
        sends.append(copy)

    def wrows(owner):
        return wfull.at[pl.ds(pl.multiple_of(owner * dblk, dblk), dblk)]

    def ccols(owner):
        return cotf.at[:, pl.ds(pl.multiple_of(owner * cshard, cshard), cshard)]

    own_w = pltpu.make_async_copy(w_ref, wrows(me), local_sem.at[0])
    own_c = pltpu.make_async_copy(cot_ref, ccols(tp), local_sem.at[1])
    loads = [
        pltpu.make_async_copy(src, dst, local_sem.at[k])
        for k, (src, dst) in enumerate(
            [(up_hbm, up_ref), (gate_hbm, gate_ref), (cw_hbm, cw_ref), (cb_hbm, cb_ref)], 2
        )
    ]

    barrier = pltpu.get_barrier_semaphore()
    peers = [((me + d) % fs_n, tp) for d in range(1, fs_n)]
    peers += [(me, ((mx + d) % x_n) * 2 + mc) for d in range(1, x_n)] + [(me, mate)]
    for peer in peers:
        pl.semaphore_signal(barrier, inc=1, device_id=peer, device_id_type=MESH)
    for copy in loads:
        copy.start()
    pl.semaphore_wait(barrier, len(peers))

    @pl.when(me < fs_n - 1)
    def _():
        rcopy(up_hbm.at[pl.ds(rows - 16, 16)], halo_up, hu_sem.at[0], hu_sem.at[1], me + 1, tp).start()

    for d in range(1, x_n):
        send(cot_ref, ccols(tp), c_send_x.at[d], c_recv.at[tp], me, ((mx + d) % x_n) * 2 + mc)
    for d in range(1, z_n):
        send(w_ref, wrows(me), w_send_z.at[d], w_recv.at[me], ((mz + d) % z_n) * y_n + my, tp)
    for d in range(1, y_n):
        send(w_ref, wrows(me), w_send_y.at[d], w_recv.at[me], mz * y_n + (my + d) % y_n, tp)
    send(cot_ref, ccols(tp), c_send_m.at[0], c_recv.at[tp], me, mate)
    own_w.start()
    own_c.start()

    for copy in loads:
        copy.wait()

    @pl.when(me > 0)
    def _():
        rcopy(halo_up, halo_up, hu_sem.at[0], hu_sem.at[1], me - 1, tp).wait_recv()
        upf[0:8] = halo_up[...].astype(F32)[8:16]

    @pl.when(me == 0)
    def _():
        upf[0:8] = jnp.zeros((8, cols), F32)

    upf[8 : rows + 8] = up_ref[...].astype(F32)
    step = 64

    @pl.loop(0, cols // 128)
    def _(j):
        lanes = pl.ds(pl.multiple_of(j * 128, 128), 128)
        taps = [cw_ref[k : k + 1, lanes] for k in range(3)]
        bias = cb_ref[0:1, lanes]
        for r in range(0, rows, step):
            conv = bias + taps[0] * upf[r + 6 : r + 6 + step, lanes]
            conv = conv + taps[1] * upf[r + 7 : r + 7 + step, lanes]
            conv = conv + taps[2] * upf[r + 8 : r + 8 + step, lanes]
            sig = 1.0 / (1.0 + jnp.exp(-conv))
            a = conv * sig
            g = gate_ref[r : r + step, lanes].astype(F32)
            act[r : r + step, lanes] = a
            hidden[r : r + step, lanes] = (a * g).astype(BF16)
            gfac[r : r + step, lanes] = g * sig * (1.0 + conv * (1.0 - sig))

    def wait_cot(d, other):
        owner = ((mx + x_n - d) % x_n) * 2 + (1 - mc if other else mc)
        sem = c_send_m if other else c_send_x
        rcopy(cot_ref, ccols(owner), sem.at[d], c_recv.at[owner], me, mate if other else owner).wait_recv()
        return owner

    ywide = y_n * dblk
    tile = min(256, cols)
    own_chunks = max(z_n // x_n, 1)

    def chunk(o):
        return (mx * own_chunks + o) % z_n

    def partial_grad(o):
        zp = chunk(o)
        base = pl.multiple_of(zp * ywide, ywide)
        lhs_t[...] = cotf[:, pl.ds(base, ywide)].T

        @pl.loop(0, cols // tile)
        def _(j):
            lanes = pl.ds(pl.multiple_of(j * tile, tile), tile)
            out = jnp.dot(lhs_t[...], hidden[:, lanes], preferred_element_type=F32)
            pf32[pl.ds(base, ywide), lanes] = out
            pbf[pl.ds(base, ywide), lanes] = out.astype(BF16)

        for e in range(1, y_n):
            yp = (my + e) % y_n
            block = pl.ds(pl.multiple_of((zp * y_n + yp) * dblk, dblk), dblk)
            sem = (e - 1) * z_n + o
            send(pbf.at[block], r1.at[e - 1, o], r1_send.at[sem], r1_recv.at[sem], mz * y_n + yp, tp)

    own_c.wait()
    wait_cot(0, True)
    for o in range(own_chunks):
        partial_grad(o)
    for d in range(1, x_n):
        owner = wait_cot(d, False)
        send(ccols(owner), ccols(owner), c_send_m.at[d], c_recv.at[owner], me, mate)
    for d in range(1, x_n):
        wait_cot(d, True)
    for o in range(own_chunks, z_n):
        partial_grad(o)

    def y_sum_wait(o):
        for e in range(1, y_n):
            sem = (e - 1) * z_n + o
            rcopy(r1.at[e - 1, o], r1.at[e - 1, o], r1_send.at[sem], r1_recv.at[sem],
                  mz * y_n + (my + e) % y_n, tp).wait_recv()

    def y_sum(o, block, lanes):
        total = pf32[block, lanes]
        for e in range(1, y_n):
            total = total + r1[e - 1, o, :, lanes].astype(F32)
        return total

    def z_copy(o):
        return rcopy(s2.at[o], r2.at[mz], r2_send.at[o], r2_recv.at[mz], chunk(o) * y_n + my, tp)

    def sum_and_send(o):
        zp = chunk(o)
        block = pl.ds(pl.multiple_of((zp * y_n + my) * dblk, dblk), dblk)
        y_sum_wait(o)

        @pl.when(zp != mz)
        def _():
            @pl.loop(0, cols // 128)
            def _(j):
                lanes = pl.ds(pl.multiple_of(j * 128, 128), 128)
                s2[o, :, lanes] = y_sum(o, block, lanes).astype(BF16)

            z_copy(o).start()

    early = z_n // 2
    for o in range(early):
        sum_and_send(o)

    own_w.wait()
    for d in range(1, z_n):
        owner = ((mz + z_n - d) % z_n) * y_n + my
        rcopy(w_ref, wrows(owner), w_send_z.at[d], w_recv.at[owner], owner, tp).wait_recv()
        for e in range(1, y_n):
            send(wrows(owner), wrows(owner), w_send_y.at[d * y_n + e], w_recv.at[owner],
                 mz * y_n + (my + e) % y_n, tp)

    part_rows = 256

    def add_block(owner, first, last):
        wide = pl.multiple_of(owner * dblk, dblk)

        @pl.loop(0, cols // tile)
        def _(j):
            lanes = pl.ds(pl.multiple_of(j * tile, tile), tile)

            @pl.loop(0, rows // part_rows)
            def _(i):
                part = pl.ds(pl.multiple_of(i * part_rows, part_rows), part_rows)
                hg = jnp.dot(cotf[part, pl.ds(wide, dblk)], wfull[pl.ds(wide, dblk), lanes], preferred_element_type=F32)
                if not first:
                    hg = hg + cg[part, lanes]
                if last:
                    gg_ref[part, lanes] = (hg * act[part, lanes]).astype(BF16)
                    hg = hg * gfac[part, lanes]
                cg[part, lanes] = hg

    sum_and_send(early)
    small = dblk % 128 != 0
    if not small:
        for d in range(z_n):
            add_block(((mz + z_n - d) % z_n) * y_n + my, d == 0, False)
    for o in range(early + 1, z_n):
        sum_and_send(o)
    for d in range(z_n):
        for e in range(1, y_n):
            owner = ((mz + z_n - d) % z_n) * y_n + (my + y_n - e) % y_n
            rcopy(wrows(owner), wrows(owner), w_send_y.at[d * y_n + e], w_recv.at[owner],
                  mz * y_n + (my + e) % y_n, tp).wait_recv()
            if not small:
                add_block(owner, False, d == z_n - 1 and e == y_n - 1)
    if small:

        @pl.loop(0, cols // tile)
        def _(j):
            lanes = pl.ds(pl.multiple_of(j * tile, tile), tile)

            @pl.loop(0, rows // part_rows)
            def _(i):
                part = pl.ds(pl.multiple_of(i * part_rows, part_rows), part_rows)
                hg = jnp.dot(cotf[part, :], wfull[:, lanes], preferred_element_type=F32)
                gg_ref[part, lanes] = (hg * act[part, lanes]).astype(BF16)
                cg[part, lanes] = hg * gfac[part, lanes]

    @pl.when(me > 0)
    def _():
        rcopy(cg.at[pl.ds(0, 8)], halo_cg, hc_sem.at[0], hc_sem.at[1], me - 1, tp).start()

    @pl.loop(0, cols // 128)
    def _(j):
        lanes = pl.ds(pl.multiple_of(j * 128, 128), 128)
        sums = [jnp.zeros((8, 128), F32) for _ in range(4)]
        for r in range(0, rows, step):
            grad = cg[r : r + step, lanes]
            terms = [grad * upf[r + 6 + k : r + 6 + k + step, lanes] for k in range(3)] + [grad]
            sums = [s + jnp.sum(t.reshape(step // 8, 8, 128), axis=0) for s, t in zip(sums, terms)]
        for k in range(4):
            st[me, k : k + 1, lanes] = jnp.sum(sums[k], axis=0, keepdims=True)
        st[me, 4:8, lanes] = jnp.zeros((4, 128), F32)

    for d in range(1, fs_n):
        send(st.at[me], st.at[me], st_send.at[d], st_recv.at[me], (me + d) % fs_n, tp)

    mine = (mz + z_n - chunk(0)) % z_n
    for d in range(1, z_n):
        zp = (mz + d) % z_n
        rcopy(s2.at[0], r2.at[zp], r2_send.at[0], r2_recv.at[zp], zp * y_n + my, tp).wait_recv()
    own_block = pl.ds(pl.multiple_of(me * dblk, dblk), dblk)

    @pl.loop(0, cols // 128)
    def _(j):
        lanes = pl.ds(pl.multiple_of(j * 128, 128), 128)
        total = y_sum(mine, own_block, lanes)
        for d in range(1, z_n):
            total = total + r2[(mz + d) % z_n, :, lanes].astype(F32)
        wg_ref[:, lanes] = total
        nb[me, :, lanes] = jnp.sum(total * total, axis=0, keepdims=True)

    for d in range(1, fs_n):
        send(nb.at[me], nb.at[me], nb_send.at[d], nb_recv.at[me], (me + d) % fs_n, tp)

    @pl.when(me < fs_n - 1)
    def _():
        rcopy(halo_cg, halo_cg, hc_sem.at[0], hc_sem.at[1], me + 1, tp).wait_recv()
        cg[rows : rows + 8] = halo_cg[...]

    @pl.when(me == fs_n - 1)
    def _():
        cg[rows : rows + 8] = jnp.zeros((8, cols), F32)

    @pl.loop(0, cols // 128)
    def _(j):
        lanes = pl.ds(pl.multiple_of(j * 128, 128), 128)
        taps = [cw_ref[k : k + 1, lanes] for k in range(3)]
        for r in range(0, rows, step):
            total = taps[0] * cg[r + 2 : r + 2 + step, lanes]
            total = total + taps[1] * cg[r + 1 : r + 1 + step, lanes]
            total = total + taps[2] * cg[r : r + step, lanes]
            ug_ref[r : r + step, lanes] = total.astype(BF16)

    for d in range(1, fs_n):
        owner = (me + d) % fs_n
        rcopy(st.at[owner], st.at[owner], st_send.at[d], st_recv.at[owner], owner, tp).wait_recv()
    stats = st[0]
    for k in range(1, fs_n):
        stats = stats + st[k]
    tap_ref[...] = stats[0:3]
    bias_ref[...] = stats[3:4]
    for d in range(1, fs_n):
        owner = (me + d) % fs_n
        rcopy(nb.at[owner], nb.at[owner], nb_send.at[d], nb_recv.at[owner], owner, tp).wait_recv()
    norms = nb[0]
    for k in range(1, fs_n):
        norms = norms + nb[k]
    norm_ref[...] = norms

    for copy in sends:
        copy.wait_send()
    for o in range(z_n):

        @pl.when(chunk(o) != mz)
        def _():
            z_copy(o).wait_send()

    @pl.when(me < fs_n - 1)
    def _():
        rcopy(up_hbm.at[pl.ds(rows - 16, 16)], halo_up, hu_sem.at[0], hu_sem.at[1], me + 1, tp).wait_send()

    @pl.when(me > 0)
    def _():
        rcopy(cg.at[pl.ds(0, 8)], halo_cg, hc_sem.at[0], hc_sem.at[1], me - 1, tp).wait_send()


def general_call(fs_n, tp_n, y_n, args):
    up_pre, _, _, down_weight, _, _ = args
    rows, cols = up_pre.shape
    dblk = down_weight.shape[0]
    width = dblk * fs_n
    z_n = fs_n // y_n
    dma = pltpu.SemaphoreType.DMA
    vmem = pl.BlockSpec(memory_space=pltpu.VMEM)
    return pl.pallas_call(
        functools.partial(kernel, fs_n, tp_n, y_n),
        out_shape=(
            jax.ShapeDtypeStruct((rows, cols), BF16),
            jax.ShapeDtypeStruct((rows, cols), BF16),
            jax.ShapeDtypeStruct((dblk, cols), F32),
            jax.ShapeDtypeStruct((3, cols), F32),
            jax.ShapeDtypeStruct((1, cols), F32),
            jax.ShapeDtypeStruct((1, cols), F32),
        ),
        in_specs=[pl.BlockSpec(memory_space=pltpu.HBM)] * 6,
        out_specs=[vmem] * 6,
        scratch_shapes=[
            pltpu.VMEM((width, cols), BF16),
            pltpu.VMEM((rows, width), BF16),
            pltpu.VMEM((y_n * dblk, rows), BF16),
            pltpu.VMEM((rows, cols), BF16),
            pltpu.VMEM((rows, cols), F32),
            pltpu.VMEM((rows, cols), F32),
            pltpu.VMEM((rows + 8, cols), F32),
            pltpu.VMEM((rows + 8, cols), F32),
            pltpu.VMEM((width, cols), F32),
            pltpu.VMEM((width, cols), BF16),
            pltpu.VMEM((y_n - 1, z_n, dblk, cols), BF16),
            pltpu.VMEM((z_n, dblk, cols), BF16),
            pltpu.VMEM((z_n, dblk, cols), BF16),
            pltpu.VMEM((fs_n, 8, cols), F32),
            pltpu.VMEM((fs_n, 1, cols), F32),
            pltpu.VMEM((16, cols), BF16),
            pltpu.VMEM((8, cols), F32),
            pltpu.VMEM((rows, cols), BF16),
            pltpu.VMEM((rows, cols), BF16),
            pltpu.VMEM((3, cols), F32),
            pltpu.VMEM((1, cols), F32),
            dma((6,)),
            dma((fs_n,)), dma((z_n,)), dma((z_n * y_n,)),
            dma((tp_n,)), dma((tp_n // 2,)), dma((tp_n // 2,)),
            dma(((y_n - 1) * z_n,)), dma(((y_n - 1) * z_n,)),
            dma((z_n,)), dma((z_n,)),
            dma((fs_n,)), dma((fs_n,)), dma((fs_n,)), dma((fs_n,)),
            dma((2,)), dma((2,)),
        ],
        compiler_params=pltpu.CompilerParams(
            collective_id=0, has_side_effects=True, vmem_limit_bytes=48000 * 1024
        ),
    )(*args)


def line_kernel(
    fs_n, tp_n, y_n, n1,
    up_hbm, gate_hbm, cot_hbm, w_hbm, cw_hbm, cb_hbm,
    ug_ref, gg_ref, wg_ref, tap_ref, bias_ref, norm_ref,
    wfull, cotf, lhs_t, hidden, act, gfac, upf, cg, pf32,
    ysend, yrecv, sz1, rz1, sz2, rz2, sf, rf,
    sy, st, nb, halo_up, halo_cg, cw_ref, cb_ref,
    local_sem, ag_send, ag_recv, yw_send, yw_recv, yp_sem, c_send, c_recv, ry_send, ry_recv,
    rs_send, rs_recv, f_sem, st_recv, st_send, nb_recv, nb_send, hu_sem, hc_sem,
):
    rows, cols = up_hbm.shape
    dblk = w_hbm.shape[0]
    cshard = cot_hbm.shape[1]
    ywide = y_n * dblk
    z_n = fs_n // y_n
    n2 = cols - n1
    me, tp = lax.axis_index("fs"), lax.axis_index("tp")
    mz, my = me // y_n, me % y_n
    mx, mc = tp // 2, tp % 2
    mate = mx * 2 + (1 - mc)
    mirror = (1 - mx) * 2 + mc
    ynb = mz * y_n + (1 - my)
    sign = (1, -1)
    avail = (mz, z_n - 1 - mz)
    has_next = (mz < z_n - 1, mz > 0)
    has_prev = (mz > 0, mz < z_n - 1)
    nxt = [((mz + z_n + s) % z_n) * y_n + my for s in sign]
    sends = []

    def rcopy(src, dst, ss, rs, fs_id, tp_id):
        return pltpu.make_async_remote_copy(
            src_ref=src, dst_ref=dst, send_sem=ss, recv_sem=rs,
            device_id=(fs_id, tp_id), device_id_type=MESH,
        )

    def start(make, pred=None, inside=None):
        if pred is None:
            make().start()
        else:
            @pl.when(pred if inside is None else inside)
            def _():
                make().start()
        sends.append((pred, make))

    def drows(zp, y):
        return pl.ds(pl.multiple_of((zp * y_n + y) * dblk, dblk), dblk)

    half_rows = rows // 2

    def ccols(owner):
        return cotf.at[:, pl.ds(pl.multiple_of(owner * cshard, cshard), cshard)]

    def chalf(owner, half):
        tokens = pl.ds(pl.multiple_of(half * half_rows, half_rows), half_rows)
        return cotf.at[tokens, pl.ds(pl.multiple_of(owner * cshard, cshard), cshard)]

    def urgent(side):
        outer = side * (z_n - 1)
        return jnp.where(mz == outer, side * (z_n // 2) + 1 - side, outer)

    def other(side, quarter):
        return 2 * side * (z_n // 2) + 1 - quarter

    def cx_copy(order, src=None):
        quarter = urgent(mx) if order == 0 else other(mx, urgent(mx))
        ref = chalf(quarter, mc)
        return rcopy(ref if src is None else src, ref, c_send.at[order], c_recv.at[order], me, mirror)

    def cm_copy(order, half):
        quarter = urgent(1 - mx) if order == 0 else other(1 - mx, urgent(1 - mx))
        ref = chalf(quarter, half)
        return rcopy(ref, ref, c_send.at[2 + order], c_recv.at[2 + order], me, mate)

    part1, part2 = pl.ds(0, n1), pl.ds(n1, n2)

    def ag_copy(d, slot, part, zp):
        ref = wfull.at[drows(zp, 1 - my if part == 2 else my), part1 if part == 1 else part2]
        src = ref
        if slot == 0 and part < 2:
            src = w_hbm.at[:, part1 if part == 1 else part2]
        i = (d * z_n + slot) * 3 + part
        return rcopy(src, ref, ag_send.at[i], ag_recv.at[i], nxt[d], tp)

    def yw_copy(zp, own=False):
        ref = wfull.at[drows(zp, my), part1]
        return rcopy(w_hbm.at[:, part1] if own else ref, ref, yw_send.at[zp], yw_recv.at[zp], ynb, tp)

    def yw_wait(zp):
        ref = wfull.at[drows(zp, 1 - my), part1]
        rcopy(ref, ref, yw_send.at[zp], yw_recv.at[zp], ynb, tp).wait_recv()

    def rs_copy(d, slot, part, t):
        i = (d * z_n + slot) * 2 + part
        slot_to = z_n if d == 1 and slot == z_n - 1 else t
        src, dst = (sz2.at[t], rz2.at[slot_to]) if part == 0 else (sz1.at[t], rz1.at[slot_to])
        return rcopy(src, dst, rs_send.at[i], rs_recv.at[i], nxt[d], tp)

    def ry_copy(t):
        return rcopy(ysend.at[t], yrecv.at[t], ry_send.at[t], ry_recv.at[t], ynb, tp)

    own_w = pltpu.make_async_copy(w_hbm, wfull.at[drows(mz, my)], local_sem.at[0])
    own_c = pltpu.make_async_copy(cot_hbm, ccols(tp), local_sem.at[1])
    loads = [
        pltpu.make_async_copy(src, dst, local_sem.at[k])
        for k, (src, dst) in enumerate(
            [(up_hbm, ug_ref), (gate_hbm, gg_ref), (cw_hbm, cw_ref), (cb_hbm, cb_ref)], 2
        )
    ]

    barrier = pltpu.get_barrier_semaphore()
    peers = [((me + d) % fs_n, tp) for d in range(1, fs_n)] + [(me, mirror), (me, mate)]
    for peer in peers:
        pl.semaphore_signal(barrier, inc=1, device_id=peer, device_id_type=MESH)
    for copy in loads:
        copy.start()
    own_c.start()
    own_w.start()
    pl.semaphore_wait(barrier, len(peers))

    start(
        lambda: rcopy(up_hbm.at[pl.ds(rows - 16, 16)], halo_up, hu_sem.at[0], hu_sem.at[1], (me + 1) % fs_n, tp),
        me < fs_n - 1,
    )
    yp_copy = lambda: rcopy(
        w_hbm.at[:, part2], wfull.at[drows(mz, my), part2], yp_sem.at[0], yp_sem.at[1], ynb, tp
    )
    start(yp_copy)
    for part in (0, 1):
        for d in (0, 1):
            start(functools.partial(ag_copy, d, 0, part, mz), has_next[d])
    start(functools.partial(yw_copy, mz, True))
    start(lambda: rcopy(cot_hbm, ccols(tp), c_send.at[4], c_recv.at[4], me, mate))
    own_half = cot_hbm.at[pl.ds(pl.multiple_of(mc * half_rows, half_rows), half_rows)]
    leads = urgent(mx) == tp

    @pl.when(leads)
    def _():
        cx_copy(0, own_half).start()

    rcopy(cot_hbm, ccols(mate), c_send.at[4], c_recv.at[4], me, mate).wait_recv()

    @pl.when(leads)
    def _():
        cx_copy(1).start()

    @pl.when(jnp.logical_not(leads))
    def _():
        cx_copy(0).start()
        cx_copy(1, own_half).start()

    sends.append((None, functools.partial(cx_copy, 0)))
    sends.append((None, functools.partial(cx_copy, 1)))

    for copy in loads:
        copy.wait()

    upf[8 : rows + 8] = ug_ref[...].astype(F32)
    step = 64

    def conv_rows(first, end):
        @pl.loop(0, cols // 128)
        def _(j):
            lanes = pl.ds(pl.multiple_of(j * 128, 128), 128)
            taps = [cw_ref[k : k + 1, lanes] for k in range(3)]
            bias = cb_ref[0:1, lanes]
            for r in range(first, end, step):
                conv = bias + taps[0] * upf[r + 6 : r + 6 + step, lanes]
                conv = conv + taps[1] * upf[r + 7 : r + 7 + step, lanes]
                conv = conv + taps[2] * upf[r + 8 : r + 8 + step, lanes]
                sig = 1.0 / (1.0 + jnp.exp(-conv))
                a = conv * sig
                g = gg_ref[r : r + step, lanes].astype(F32)
                act[r : r + step, lanes] = a
                hidden[r : r + step, lanes] = (a * g).astype(BF16)
                gfac[r : r + step, lanes] = g * sig * (1.0 + conv * (1.0 - sig))

    conv_rows(step, rows)

    @pl.when(me > 0)
    def _():
        rcopy(halo_up, halo_up, hu_sem.at[0], hu_sem.at[1], (me + fs_n - 1) % fs_n, tp).wait_recv()
        upf[0:8] = halo_up[...].astype(F32)[8:16]

    @pl.when(me == 0)
    def _():
        upf[0:8] = jnp.zeros((8, cols), F32)

    conv_rows(0, step)

    rcopy(
        w_hbm.at[:, part2], wfull.at[drows(mz, 1 - my), part2], yp_sem.at[0], yp_sem.at[1], ynb, tp
    ).wait_recv()
    for d in (0, 1):
        start(functools.partial(ag_copy, d, 0, 2, mz), has_next[d])

    tile = min(256, cols)

    def wg_part(t):
        base = pl.multiple_of(t * ywide, ywide)
        lhs_t[...] = cotf[:, pl.ds(base, ywide)].T

        @pl.loop(0, cols // tile)
        def _(j):
            lanes = pl.ds(pl.multiple_of(j * tile, tile), tile)
            pf32[pl.ds(base, ywide), lanes] = jnp.dot(lhs_t[...], hidden[:, lanes], preferred_element_type=F32)

        @pl.loop(0, n1 // 128)
        def _(j):
            lanes = pl.ds(pl.multiple_of(j * 128, 128), 128)
            ysend[t, :, lanes] = pf32[drows(t, 1 - my), lanes].astype(BF16)

    first, second = urgent(mx), urgent(1 - mx)
    third, fourth = other(mx, first), other(1 - mx, second)

    def ry_start(t, delta=None):
        pred = None if delta is None else jnp.abs(t - mz) == delta
        start(functools.partial(ry_copy, t), pred)

    def wg_far(order):
        cx = fourth if order else second
        rcopy(chalf(cx, mc), chalf(cx, mc), c_send.at[order], c_recv.at[order], me, mirror).wait_recv()
        start(functools.partial(cm_copy, order, mc))
        cm_copy(order, 1 - mc).wait_recv()
        wg_part(cx)

    own_c.wait()
    wg_part(first)
    ry_start(first)
    wg_far(0)
    ry_start(second, z_n - 1)
    def ag_step(k, part):
        for d in (0, 1):
            zp = (mz + z_n - sign[d] * (1 + k)) % z_n
            is_ag = k < avail[d]

            @pl.when(is_ag)
            def _():
                ag_copy(d, k, part, zp).wait_recv()
                if k + 1 < z_n - 1:
                    @pl.when(has_next[d])
                    def _():
                        ag_copy(d, k + 1, part, zp).start()
                if part == 1:
                    yw_copy(zp).start()

            if k + 1 < z_n - 1:
                sends.append((is_ag & has_next[d], functools.partial(ag_copy, d, k + 1, part, zp)))
            if part == 1:
                sends.append((is_ag, functools.partial(yw_copy, zp)))

    def rs_step(k, part):
        for d in (0, 1):
            t = (mz + z_n - sign[d] * (1 + k)) % z_n
            pred = k >= avail[d]

            def run(arrived, d=d, t=t):
                if part == 1:
                    ry_copy(t).wait_recv()
                if arrived:
                    rs_copy(d, k, part, t).wait_recv()

                @pl.loop(0, (n1 if part else n2) // 128)
                def _(j):
                    near = pl.ds(pl.multiple_of(j * 128, 128), 128)
                    if part == 1:
                        total = pf32[drows(t, my), near] + yrecv[t, :, near].astype(F32)
                    else:
                        far = pl.ds(pl.multiple_of(n1 + j * 128, 128), 128)
                        total = pf32[pl.ds(pl.multiple_of(t * ywide, ywide), ywide), far]
                    if arrived:
                        total = total + (rz1 if part else rz2)[t, :, near].astype(F32)
                    (sz1 if part else sz2)[t, :, near] = total.astype(BF16)

                rs_copy(d, k + 1, part, t).start()

            if k > 0:
                pl.when(pred & has_prev[d])(functools.partial(run, True))
            pl.when(pred & jnp.logical_not(has_prev[d]))(functools.partial(run, False))
            sends.append((pred, functools.partial(rs_copy, d, k + 1, part, t)))

    part_rows = rows // 2 if rows % 32 == 0 else rows

    def hg_add(zp, first):
        base = pl.ds(pl.multiple_of(zp * ywide, ywide), ywide)

        @pl.loop(0, cols // tile)
        def _(j):
            lanes = pl.ds(pl.multiple_of(j * tile, tile), tile)

            @pl.loop(0, rows // part_rows)
            def _(i):
                part = pl.ds(pl.multiple_of(i * part_rows, part_rows), part_rows)
                hg = jnp.dot(cotf[part, base], wfull[base, lanes], preferred_element_type=F32)
                if not first:
                    hg = hg + cg[part, lanes]
                cg[part, lanes] = hg

    def hg_far(delta):
        for s in sign:
            zp = mz + s * delta

            @pl.when((zp >= 0) & (zp < z_n))
            def _():
                near = (zp + z_n) % z_n
                yw_wait(near)
                hg_add(near, False)

    ag_step(0, 0)
    ag_step(0, 1)
    for delta in range(z_n - 2, 1, -1):
        ry_start(second, delta)
    rs_step(0, 0)
    wg_part(third)
    for delta in range(z_n - 2, 1, -1):
        ry_start(third, delta)
    ag_step(0, 2)
    wg_far(1)
    for delta in range(z_n - 2, 1, -1):
        ry_start(fourth, delta)
    own_w.wait()
    yw_wait(mz)
    hg_add(mz, True)
    rs_step(0, 1)
    ag_step(1, 0)
    ag_step(1, 1)
    for t in (second, third, fourth):
        ry_start(t, 1)
    rs_step(1, 0)
    ag_step(1, 2)
    rs_step(1, 1)
    hg_far(1)
    ag_step(2, 0)
    ag_step(2, 1)
    for t in (second, third, fourth):
        ry_start(t, 0)
    rs_step(2, 0)
    ag_step(2, 2)
    rs_step(2, 1)
    hg_far(2)
    hg_far(z_n - 1)

    @pl.loop(0, cols // 128)
    def _(j):
        lanes = pl.ds(pl.multiple_of(j * 128, 128), 128)
        for r in range(0, rows, step):
            part = slice(r, r + step)
            hg = cg[part, lanes]
            gg_ref[part, lanes] = (hg * act[part, lanes]).astype(BF16)
            cg[part, lanes] = hg * gfac[part, lanes]

    start(
        lambda: rcopy(cg.at[pl.ds(0, 8)], halo_cg, hc_sem.at[0], hc_sem.at[1], (me + fs_n - 1) % fs_n, tp),
        me > 0,
    )

    @pl.loop(0, cols // 128)
    def _(j):
        lanes = pl.ds(pl.multiple_of(j * 128, 128), 128)
        sums = [jnp.zeros((8, 128), F32) for _ in range(4)]
        for r in range(0, rows, step):
            grad = cg[r : r + step, lanes]
            terms = [grad * upf[r + 6 + k : r + 6 + k + step, lanes] for k in range(3)] + [grad]
            sums = [s + jnp.sum(t.reshape(step // 8, 8, 128), axis=0) for s, t in zip(sums, terms)]
        for k in range(4):
            sy[my, k : k + 1, lanes] = jnp.sum(sums[k], axis=0, keepdims=True)

    start(lambda: rcopy(sy.at[my], sy.at[my], st_send.at[0], st_recv.at[z_n], ynb, tp))

    last = z_n - 1
    for d in (0, 1):

        @pl.when(has_prev[d])
        def _():
            rs_copy(d, last, 0, mz).wait_recv()

            @pl.loop(0, n2 // 128)
            def _(j):
                far = pl.ds(pl.multiple_of(n1 + j * 128, 128), 128)
                near = pl.ds(pl.multiple_of(j * 128, 128), 128)
                block = pl.ds(pl.multiple_of(mz * ywide, ywide), ywide)
                pf32[block, far] = pf32[block, far] + rz2[z_n if d == 1 else mz, :, near].astype(F32)

    @pl.loop(0, n2 // 128)
    def _(j):
        far = pl.ds(pl.multiple_of(n1 + j * 128, 128), 128)
        near = pl.ds(pl.multiple_of(j * 128, 128), 128)
        sf[:, near] = pf32[drows(mz, 1 - my), far].astype(BF16)

    f_copy = lambda: rcopy(sf, rf, f_sem.at[0], f_sem.at[1], ynb, tp)
    start(f_copy)

    rcopy(sy.at[1 - my], sy.at[1 - my], st_send.at[0], st_recv.at[z_n], ynb, tp).wait_recv()
    st[mz] = sy[0] + sy[1]
    for d in range(1, z_n):
        start(
            lambda d=d: rcopy(
                st.at[mz], st.at[mz], st_send.at[d], st_recv.at[mz], ((mz + d) % z_n) * y_n + my, tp
            )
        )

    own_block = drows(mz, my)
    ry_copy(mz).wait_recv()

    @pl.loop(0, n1 // 128)
    def _(j):
        lanes = pl.ds(pl.multiple_of(j * 128, 128), 128)
        wg_ref[:, lanes] = pf32[own_block, lanes] + yrecv[mz, :, lanes].astype(F32)

    for d in (0, 1):

        @pl.when(has_prev[d])
        def _():
            rs_copy(d, last, 1, mz).wait_recv()

            @pl.loop(0, n1 // 128)
            def _(j):
                lanes = pl.ds(pl.multiple_of(j * 128, 128), 128)
                wg_ref[:, lanes] = wg_ref[:, lanes] + rz1[z_n if d == 1 else mz, :, lanes].astype(F32)

    f_copy().wait_recv()

    @pl.loop(0, n2 // 128)
    def _(j):
        far = pl.ds(pl.multiple_of(n1 + j * 128, 128), 128)
        near = pl.ds(pl.multiple_of(j * 128, 128), 128)
        wg_ref[:, far] = pf32[own_block, far] + rf[:, near].astype(F32)

    @pl.loop(0, cols // 128)
    def _(j):
        lanes = pl.ds(pl.multiple_of(j * 128, 128), 128)
        total = wg_ref[:, lanes]
        nb[me, :, lanes] = jnp.sum(total * total, axis=0, keepdims=True)

    for d in range(1, fs_n):
        start(
            lambda d=d: rcopy(nb.at[me], nb.at[me], nb_send.at[d], nb_recv.at[me], (me + d) % fs_n, tp)
        )

    @pl.when(me < fs_n - 1)
    def _():
        rcopy(halo_cg, halo_cg, hc_sem.at[0], hc_sem.at[1], (me + 1) % fs_n, tp).wait_recv()
        cg[rows : rows + 8] = halo_cg[...]

    @pl.when(me == fs_n - 1)
    def _():
        cg[rows : rows + 8] = jnp.zeros((8, cols), F32)

    @pl.loop(0, cols // 128)
    def _(j):
        lanes = pl.ds(pl.multiple_of(j * 128, 128), 128)
        taps = [cw_ref[k : k + 1, lanes] for k in range(3)]
        for r in range(0, rows, step):
            total = taps[0] * cg[r + 2 : r + 2 + step, lanes]
            total = total + taps[1] * cg[r + 1 : r + 1 + step, lanes]
            total = total + taps[2] * cg[r : r + step, lanes]
            ug_ref[r : r + step, lanes] = total.astype(BF16)

    for d in range(1, z_n):
        zp = (mz + d) % z_n
        rcopy(st.at[zp], st.at[zp], st_send.at[d], st_recv.at[zp], zp * y_n + my, tp).wait_recv()
    stats = st[0]
    for d in range(1, z_n):
        stats = stats + st[d]
    tap_ref[...] = stats[0:3]
    bias_ref[...] = stats[3:4]

    for pred, make in sends:
        if pred is None:
            make().wait_send()
        else:
            @pl.when(pred)
            def _():
                make().wait_send()

    for d in range(1, fs_n):
        owner = (me + d) % fs_n
        rcopy(nb.at[owner], nb.at[owner], nb_send.at[d], nb_recv.at[owner], owner, tp).wait_recv()
    norms = nb[0]
    for k in range(1, fs_n):
        norms = norms + nb[k]
    norm_ref[...] = norms


def line_call(fs_n, tp_n, y_n, args):
    up_pre, _, _, down_weight, _, _ = args
    rows, cols = up_pre.shape
    dblk = down_weight.shape[0]
    width = dblk * fs_n
    ywide = y_n * dblk
    z_n = fs_n // y_n
    n2 = max(cols * 3 // 8 // 128, 1) * 128
    n1 = cols - n2
    dma = pltpu.SemaphoreType.DMA
    vmem = pl.BlockSpec(memory_space=pltpu.VMEM)
    return pl.pallas_call(
        functools.partial(line_kernel, fs_n, tp_n, y_n, n1),
        out_shape=(
            jax.ShapeDtypeStruct((rows, cols), BF16),
            jax.ShapeDtypeStruct((rows, cols), BF16),
            jax.ShapeDtypeStruct((dblk, cols), F32),
            jax.ShapeDtypeStruct((3, cols), F32),
            jax.ShapeDtypeStruct((1, cols), F32),
            jax.ShapeDtypeStruct((1, cols), F32),
        ),
        in_specs=[pl.BlockSpec(memory_space=pltpu.HBM)] * 6,
        out_specs=[vmem] * 6,
        scratch_shapes=[
            pltpu.VMEM((width, cols), BF16),
            pltpu.VMEM((rows, width), BF16),
            pltpu.VMEM((ywide, rows), BF16),
            pltpu.VMEM((rows, cols), BF16),
            pltpu.VMEM((rows, cols), F32),
            pltpu.VMEM((rows, cols), F32),
            pltpu.VMEM((rows + 8, cols), F32),
            pltpu.VMEM((rows + 8, cols), F32),
            pltpu.VMEM((width, cols), F32),
            pltpu.VMEM((z_n, dblk, n1), BF16),
            pltpu.VMEM((z_n, dblk, n1), BF16),
            pltpu.VMEM((z_n, dblk, n1), BF16),
            pltpu.VMEM((z_n + 1, dblk, n1), BF16),
            pltpu.VMEM((z_n, ywide, n2), BF16),
            pltpu.VMEM((z_n + 1, ywide, n2), BF16),
            pltpu.VMEM((dblk, n2), BF16),
            pltpu.VMEM((dblk, n2), BF16),
            pltpu.VMEM((y_n, 4, cols), F32),
            pltpu.VMEM((z_n, 4, cols), F32),
            pltpu.VMEM((fs_n, 1, cols), F32),
            pltpu.VMEM((16, cols), BF16),
            pltpu.VMEM((8, cols), F32),
            pltpu.VMEM((3, cols), F32),
            pltpu.VMEM((1, cols), F32),
            dma((6,)),
            dma((6 * z_n,)), dma((6 * z_n,)), dma((z_n,)), dma((z_n,)), dma((2,)),
            dma((5,)), dma((5,)), dma((z_n,)), dma((z_n,)),
            dma((4 * z_n,)), dma((4 * z_n,)), dma((2,)),
            dma((fs_n,)), dma((z_n,)), dma((fs_n,)), dma((fs_n,)),
            dma((2,)), dma((2,)),
        ],
        compiler_params=pltpu.CompilerParams(
            collective_id=0, has_side_effects=True, vmem_limit_bytes=46000 * 1024
        ),
    )(*args)


def per_device(fs_n, tp_n, up_pre, gate_value, out_cotangent, down_weight, conv_weight, conv_bias):
    rows, cols = up_pre.shape
    dblk = down_weight.shape[0]
    width = dblk * fs_n
    y_n = max(tp_n // 2, 2)
    z_n = fs_n // y_n
    args = tuple(
        pltpu.with_memory_space_constraint(value, pltpu.HBM)
        for value in (up_pre, gate_value, out_cotangent, down_weight, conv_weight, conv_bias[None, :])
    )
    if tp_n == 4 and z_n == tp_n and rows % 64 == 0 and cols % 256 == 0 and dblk % 128 == 0:
        outs = line_call(fs_n, tp_n, y_n, args)
    else:
        outs = general_call(fs_n, tp_n, y_n, args)
    ug, gg, wg, tap, bias, norm = outs
    return ug, gg, wg, tap, bias[0], norm[0]


def solution(mesh):
    return jax.shard_map(
        functools.partial(per_device, mesh.shape["fs"], mesh.shape["tp"]),
        mesh=mesh,
        in_specs=(
            P("fs", "tp"),
            P("fs", "tp"),
            P("fs", "tp"),
            P("fs", "tp"),
            P(None, "tp"),
            P("tp"),
        ),
        out_specs=(P("fs", "tp"), P("fs", "tp"), P("fs", "tp"), P(None, "tp"), P("tp"), P("tp")),
        check_vma=False,
    )
```

```python
import functools

import jax
import jax.numpy as jnp
from jax import lax
from jax.experimental import pallas as pl
from jax.experimental.pallas import tpu as pltpu
from jax.sharding import PartitionSpec as P

MESH = pl.DeviceIdType.MESH
F32 = jnp.float32
BF16 = jnp.bfloat16


def kernel(
    fs_n, tp_n, y_n,
    up_hbm, gate_hbm, cot_ref, w_ref, cw_hbm, cb_hbm,
    ug_ref, gg_ref, wg_ref, tap_ref, bias_ref, norm_ref,
    wfull, cotf, lhs_t, hidden, act, gfac, upf, cg, pf32, pbf,
    r1, s2, r2, st, nb, halo_up, halo_cg, up_ref, gate_ref, cw_ref, cb_ref,
    local_sem, w_recv, w_send_z, w_send_y, c_recv, c_send_x, c_send_m,
    r1_recv, r1_send, r2_recv, r2_send, st_recv, st_send, nb_recv, nb_send,
    hu_sem, hc_sem,
):
    rows, cols = up_hbm.shape
    dblk = w_ref.shape[0]
    cshard = cot_ref.shape[1]
    z_n = fs_n // y_n
    x_n = tp_n // 2
    me, tp = lax.axis_index("fs"), lax.axis_index("tp")
    mz, my = me // y_n, me % y_n
    mx, mc = tp // 2, tp % 2
    mate = mx * 2 + (1 - mc)
    sends = []

    def rcopy(src, dst, ss, rs, fs_id, tp_id):
        return pltpu.make_async_remote_copy(
            src_ref=src, dst_ref=dst, send_sem=ss, recv_sem=rs,
            device_id=(fs_id, tp_id), device_id_type=MESH,
        )

    def send(*args):
        copy = rcopy(*args)
        copy.start()
        sends.append(copy)

    def wrows(owner):
        return wfull.at[pl.ds(pl.multiple_of(owner * dblk, dblk), dblk)]

    def ccols(owner):
        return cotf.at[:, pl.ds(pl.multiple_of(owner * cshard, cshard), cshard)]

    own_w = pltpu.make_async_copy(w_ref, wrows(me), local_sem.at[0])
    own_c = pltpu.make_async_copy(cot_ref, ccols(tp), local_sem.at[1])
    loads = [
        pltpu.make_async_copy(src, dst, local_sem.at[k])
        for k, (src, dst) in enumerate(
            [(up_hbm, up_ref), (gate_hbm, gate_ref), (cw_hbm, cw_ref), (cb_hbm, cb_ref)], 2
        )
    ]

    barrier = pltpu.get_barrier_semaphore()
    peers = [((me + d) % fs_n, tp) for d in range(1, fs_n)]
    peers += [(me, ((mx + d) % x_n) * 2 + mc) for d in range(1, x_n)] + [(me, mate)]
    for peer in peers:
        pl.semaphore_signal(barrier, inc=1, device_id=peer, device_id_type=MESH)
    for copy in loads:
        copy.start()
    pl.semaphore_wait(barrier, len(peers))

    @pl.when(me < fs_n - 1)
    def _():
        rcopy(up_hbm.at[pl.ds(rows - 16, 16)], halo_up, hu_sem.at[0], hu_sem.at[1], me + 1, tp).start()

    for d in range(1, x_n):
        send(cot_ref, ccols(tp), c_send_x.at[d], c_recv.at[tp], me, ((mx + d) % x_n) * 2 + mc)
    for d in range(1, z_n):
        send(w_ref, wrows(me), w_send_z.at[d], w_recv.at[me], ((mz + d) % z_n) * y_n + my, tp)
    for d in range(1, y_n):
        send(w_ref, wrows(me), w_send_y.at[d], w_recv.at[me], mz * y_n + (my + d) % y_n, tp)
    send(cot_ref, ccols(tp), c_send_m.at[0], c_recv.at[tp], me, mate)
    own_w.start()
    own_c.start()

    for copy in loads:
        copy.wait()

    @pl.when(me > 0)
    def _():
        rcopy(halo_up, halo_up, hu_sem.at[0], hu_sem.at[1], me - 1, tp).wait_recv()
        upf[0:8] = halo_up[...].astype(F32)[8:16]

    @pl.when(me == 0)
    def _():
        upf[0:8] = jnp.zeros((8, cols), F32)

    upf[8 : rows + 8] = up_ref[...].astype(F32)
    step = 64

    @pl.loop(0, cols // 128)
    def _(j):
        lanes = pl.ds(pl.multiple_of(j * 128, 128), 128)
        taps = [cw_ref[k : k + 1, lanes] for k in range(3)]
        bias = cb_ref[0:1, lanes]
        for r in range(0, rows, step):
            conv = bias + taps[0] * upf[r + 6 : r + 6 + step, lanes]
            conv = conv + taps[1] * upf[r + 7 : r + 7 + step, lanes]
            conv = conv + taps[2] * upf[r + 8 : r + 8 + step, lanes]
            sig = 1.0 / (1.0 + jnp.exp(-conv))
            a = conv * sig
            g = gate_ref[r : r + step, lanes].astype(F32)
            act[r : r + step, lanes] = a
            hidden[r : r + step, lanes] = (a * g).astype(BF16)
            gfac[r : r + step, lanes] = g * sig * (1.0 + conv * (1.0 - sig))

    def wait_cot(d, other):
        owner = ((mx + x_n - d) % x_n) * 2 + (1 - mc if other else mc)
        sem = c_send_m if other else c_send_x
        rcopy(cot_ref, ccols(owner), sem.at[d], c_recv.at[owner], me, mate if other else owner).wait_recv()
        return owner

    ywide = y_n * dblk
    tile = min(256, cols)
    own_chunks = max(z_n // x_n, 1)

    def chunk(o):
        return (mx * own_chunks + o) % z_n

    def partial_grad(o):
        zp = chunk(o)
        base = pl.multiple_of(zp * ywide, ywide)
        lhs_t[...] = cotf[:, pl.ds(base, ywide)].T

        @pl.loop(0, cols // tile)
        def _(j):
            lanes = pl.ds(pl.multiple_of(j * tile, tile), tile)
            out = jnp.dot(lhs_t[...], hidden[:, lanes], preferred_element_type=F32)
            pf32[pl.ds(base, ywide), lanes] = out
            pbf[pl.ds(base, ywide), lanes] = out.astype(BF16)

        for e in range(1, y_n):
            yp = (my + e) % y_n
            block = pl.ds(pl.multiple_of((zp * y_n + yp) * dblk, dblk), dblk)
            sem = (e - 1) * z_n + o
            send(pbf.at[block], r1.at[e - 1, o], r1_send.at[sem], r1_recv.at[sem], mz * y_n + yp, tp)

    own_c.wait()
    wait_cot(0, True)
    for o in range(own_chunks):
        partial_grad(o)
    for d in range(1, x_n):
        owner = wait_cot(d, False)
        send(ccols(owner), ccols(owner), c_send_m.at[d], c_recv.at[owner], me, mate)
    for d in range(1, x_n):
        wait_cot(d, True)
    for o in range(own_chunks, z_n):
        partial_grad(o)

    def y_sum_wait(o):
        for e in range(1, y_n):
            sem = (e - 1) * z_n + o
            rcopy(r1.at[e - 1, o], r1.at[e - 1, o], r1_send.at[sem], r1_recv.at[sem],
                  mz * y_n + (my + e) % y_n, tp).wait_recv()

    def y_sum(o, block, lanes):
        total = pf32[block, lanes]
        for e in range(1, y_n):
            total = total + r1[e - 1, o, :, lanes].astype(F32)
        return total

    def z_copy(o):
        return rcopy(s2.at[o], r2.at[mz], r2_send.at[o], r2_recv.at[mz], chunk(o) * y_n + my, tp)

    def sum_and_send(o):
        zp = chunk(o)
        block = pl.ds(pl.multiple_of((zp * y_n + my) * dblk, dblk), dblk)
        y_sum_wait(o)

        @pl.when(zp != mz)
        def _():
            @pl.loop(0, cols // 128)
            def _(j):
                lanes = pl.ds(pl.multiple_of(j * 128, 128), 128)
                s2[o, :, lanes] = y_sum(o, block, lanes).astype(BF16)

            z_copy(o).start()

    early = z_n // 2
    for o in range(early):
        sum_and_send(o)

    own_w.wait()
    for d in range(1, z_n):
        owner = ((mz + z_n - d) % z_n) * y_n + my
        rcopy(w_ref, wrows(owner), w_send_z.at[d], w_recv.at[owner], owner, tp).wait_recv()
        for e in range(1, y_n):
            send(wrows(owner), wrows(owner), w_send_y.at[d * y_n + e], w_recv.at[owner],
                 mz * y_n + (my + e) % y_n, tp)

    part_rows = 256

    def add_block(owner, first, last):
        wide = pl.multiple_of(owner * dblk, dblk)

        @pl.loop(0, cols // tile)
        def _(j):
            lanes = pl.ds(pl.multiple_of(j * tile, tile), tile)

            @pl.loop(0, rows // part_rows)
            def _(i):
                part = pl.ds(pl.multiple_of(i * part_rows, part_rows), part_rows)
                hg = jnp.dot(cotf[part, pl.ds(wide, dblk)], wfull[pl.ds(wide, dblk), lanes], preferred_element_type=F32)
                if not first:
                    hg = hg + cg[part, lanes]
                if last:
                    gg_ref[part, lanes] = (hg * act[part, lanes]).astype(BF16)
                    hg = hg * gfac[part, lanes]
                cg[part, lanes] = hg

    sum_and_send(early)
    small = dblk % 128 != 0
    if not small:
        for d in range(z_n):
            add_block(((mz + z_n - d) % z_n) * y_n + my, d == 0, False)
    for o in range(early + 1, z_n):
        sum_and_send(o)
    for d in range(z_n):
        for e in range(1, y_n):
            owner = ((mz + z_n - d) % z_n) * y_n + (my + y_n - e) % y_n
            rcopy(wrows(owner), wrows(owner), w_send_y.at[d * y_n + e], w_recv.at[owner],
                  mz * y_n + (my + e) % y_n, tp).wait_recv()
            if not small:
                add_block(owner, False, d == z_n - 1 and e == y_n - 1)
    if small:

        @pl.loop(0, cols // tile)
        def _(j):
            lanes = pl.ds(pl.multiple_of(j * tile, tile), tile)

            @pl.loop(0, rows // part_rows)
            def _(i):
                part = pl.ds(pl.multiple_of(i * part_rows, part_rows), part_rows)
                hg = jnp.dot(cotf[part, :], wfull[:, lanes], preferred_element_type=F32)
                gg_ref[part, lanes] = (hg * act[part, lanes]).astype(BF16)
                cg[part, lanes] = hg * gfac[part, lanes]

    @pl.when(me > 0)
    def _():
        rcopy(cg.at[pl.ds(0, 8)], halo_cg, hc_sem.at[0], hc_sem.at[1], me - 1, tp).start()

    @pl.loop(0, cols // 128)
    def _(j):
        lanes = pl.ds(pl.multiple_of(j * 128, 128), 128)
        sums = [jnp.zeros((8, 128), F32) for _ in range(4)]
        for r in range(0, rows, step):
            grad = cg[r : r + step, lanes]
            terms = [grad * upf[r + 6 + k : r + 6 + k + step, lanes] for k in range(3)] + [grad]
            sums = [s + jnp.sum(t.reshape(step // 8, 8, 128), axis=0) for s, t in zip(sums, terms)]
        for k in range(4):
            st[me, k : k + 1, lanes] = jnp.sum(sums[k], axis=0, keepdims=True)
        st[me, 4:8, lanes] = jnp.zeros((4, 128), F32)

    for d in range(1, fs_n):
        send(st.at[me], st.at[me], st_send.at[d], st_recv.at[me], (me + d) % fs_n, tp)

    mine = (mz + z_n - chunk(0)) % z_n
    for d in range(1, z_n):
        zp = (mz + d) % z_n
        rcopy(s2.at[0], r2.at[zp], r2_send.at[0], r2_recv.at[zp], zp * y_n + my, tp).wait_recv()
    own_block = pl.ds(pl.multiple_of(me * dblk, dblk), dblk)

    @pl.loop(0, cols // 128)
    def _(j):
        lanes = pl.ds(pl.multiple_of(j * 128, 128), 128)
        total = y_sum(mine, own_block, lanes)
        for d in range(1, z_n):
            total = total + r2[(mz + d) % z_n, :, lanes].astype(F32)
        wg_ref[:, lanes] = total
        nb[me, :, lanes] = jnp.sum(total * total, axis=0, keepdims=True)

    for d in range(1, fs_n):
        send(nb.at[me], nb.at[me], nb_send.at[d], nb_recv.at[me], (me + d) % fs_n, tp)

    @pl.when(me < fs_n - 1)
    def _():
        rcopy(halo_cg, halo_cg, hc_sem.at[0], hc_sem.at[1], me + 1, tp).wait_recv()
        cg[rows : rows + 8] = halo_cg[...]

    @pl.when(me == fs_n - 1)
    def _():
        cg[rows : rows + 8] = jnp.zeros((8, cols), F32)

    @pl.loop(0, cols // 128)
    def _(j):
        lanes = pl.ds(pl.multiple_of(j * 128, 128), 128)
        taps = [cw_ref[k : k + 1, lanes] for k in range(3)]
        for r in range(0, rows, step):
            total = taps[0] * cg[r + 2 : r + 2 + step, lanes]
            total = total + taps[1] * cg[r + 1 : r + 1 + step, lanes]
            total = total + taps[2] * cg[r : r + step, lanes]
            ug_ref[r : r + step, lanes] = total.astype(BF16)

    for d in range(1, fs_n):
        owner = (me + d) % fs_n
        rcopy(st.at[owner], st.at[owner], st_send.at[d], st_recv.at[owner], owner, tp).wait_recv()
    stats = st[0]
    for k in range(1, fs_n):
        stats = stats + st[k]
    tap_ref[...] = stats[0:3]
    bias_ref[...] = stats[3:4]
    for d in range(1, fs_n):
        owner = (me + d) % fs_n
        rcopy(nb.at[owner], nb.at[owner], nb_send.at[d], nb_recv.at[owner], owner, tp).wait_recv()
    norms = nb[0]
    for k in range(1, fs_n):
        norms = norms + nb[k]
    norm_ref[...] = norms

    for copy in sends:
        copy.wait_send()
    for o in range(z_n):

        @pl.when(chunk(o) != mz)
        def _():
            z_copy(o).wait_send()

    @pl.when(me < fs_n - 1)
    def _():
        rcopy(up_hbm.at[pl.ds(rows - 16, 16)], halo_up, hu_sem.at[0], hu_sem.at[1], me + 1, tp).wait_send()

    @pl.when(me > 0)
    def _():
        rcopy(cg.at[pl.ds(0, 8)], halo_cg, hc_sem.at[0], hc_sem.at[1], me - 1, tp).wait_send()


def general_call(fs_n, tp_n, y_n, args):
    up_pre, _, _, down_weight, _, _ = args
    rows, cols = up_pre.shape
    dblk = down_weight.shape[0]
    width = dblk * fs_n
    z_n = fs_n // y_n
    dma = pltpu.SemaphoreType.DMA
    vmem = pl.BlockSpec(memory_space=pltpu.VMEM)
    return pl.pallas_call(
        functools.partial(kernel, fs_n, tp_n, y_n),
        out_shape=(
            jax.ShapeDtypeStruct((rows, cols), BF16),
            jax.ShapeDtypeStruct((rows, cols), BF16),
            jax.ShapeDtypeStruct((dblk, cols), F32),
            jax.ShapeDtypeStruct((3, cols), F32),
            jax.ShapeDtypeStruct((1, cols), F32),
            jax.ShapeDtypeStruct((1, cols), F32),
        ),
        in_specs=[pl.BlockSpec(memory_space=pltpu.HBM)] * 6,
        out_specs=[vmem] * 6,
        scratch_shapes=[
            pltpu.VMEM((width, cols), BF16),
            pltpu.VMEM((rows, width), BF16),
            pltpu.VMEM((y_n * dblk, rows), BF16),
            pltpu.VMEM((rows, cols), BF16),
            pltpu.VMEM((rows, cols), F32),
            pltpu.VMEM((rows, cols), F32),
            pltpu.VMEM((rows + 8, cols), F32),
            pltpu.VMEM((rows + 8, cols), F32),
            pltpu.VMEM((width, cols), F32),
            pltpu.VMEM((width, cols), BF16),
            pltpu.VMEM((y_n - 1, z_n, dblk, cols), BF16),
            pltpu.VMEM((z_n, dblk, cols), BF16),
            pltpu.VMEM((z_n, dblk, cols), BF16),
            pltpu.VMEM((fs_n, 8, cols), F32),
            pltpu.VMEM((fs_n, 1, cols), F32),
            pltpu.VMEM((16, cols), BF16),
            pltpu.VMEM((8, cols), F32),
            pltpu.VMEM((rows, cols), BF16),
            pltpu.VMEM((rows, cols), BF16),
            pltpu.VMEM((3, cols), F32),
            pltpu.VMEM((1, cols), F32),
            dma((6,)),
            dma((fs_n,)), dma((z_n,)), dma((z_n * y_n,)),
            dma((tp_n,)), dma((tp_n // 2,)), dma((tp_n // 2,)),
            dma(((y_n - 1) * z_n,)), dma(((y_n - 1) * z_n,)),
            dma((z_n,)), dma((z_n,)),
            dma((fs_n,)), dma((fs_n,)), dma((fs_n,)), dma((fs_n,)),
            dma((2,)), dma((2,)),
        ],
        compiler_params=pltpu.CompilerParams(
            collective_id=0, has_side_effects=True, vmem_limit_bytes=48000 * 1024
        ),
    )(*args)


def line_kernel(
    fs_n, tp_n, y_n, n1,
    up_hbm, gate_hbm, cot_hbm, w_hbm, cw_hbm, cb_hbm,
    ug_ref, gg_ref, wg_ref, tap_ref, bias_ref, norm_ref,
    wfull, cotf, lhs_t, hidden, act, gfac, upf, cg, pf32,
    ysend, yrecv, sz1, rz1, sz2, rz2, sf, rf,
    sy, st, nb, halo_up, halo_cg, cw_ref, cb_ref,
    local_sem, ag_send, ag_recv, yw_send, yw_recv, yp_sem, c_send, c_recv, ry_send, ry_recv,
    rs_send, rs_recv, f_sem, st_recv, st_send, nb_recv, nb_send, hu_sem, hc_sem,
):
    rows, cols = up_hbm.shape
    dblk = w_hbm.shape[0]
    cshard = cot_hbm.shape[1]
    ywide = y_n * dblk
    z_n = fs_n // y_n
    n2 = cols - n1
    me, tp = lax.axis_index("fs"), lax.axis_index("tp")
    mz, my = me // y_n, me % y_n
    mx, mc = tp // 2, tp % 2
    mate = mx * 2 + (1 - mc)
    mirror = (1 - mx) * 2 + mc
    ynb = mz * y_n + (1 - my)
    sign = (1, -1)
    avail = (mz, z_n - 1 - mz)
    has_next = (mz < z_n - 1, mz > 0)
    has_prev = (mz > 0, mz < z_n - 1)
    nxt = [((mz + z_n + s) % z_n) * y_n + my for s in sign]
    sends = []

    def rcopy(src, dst, ss, rs, fs_id, tp_id):
        return pltpu.make_async_remote_copy(
            src_ref=src, dst_ref=dst, send_sem=ss, recv_sem=rs,
            device_id=(fs_id, tp_id), device_id_type=MESH,
        )

    def start(make, pred=None, inside=None):
        if pred is None:
            make().start()
        else:
            @pl.when(pred if inside is None else inside)
            def _():
                make().start()
        sends.append((pred, make))

    def drows(zp, y):
        return pl.ds(pl.multiple_of((zp * y_n + y) * dblk, dblk), dblk)

    half_rows = rows // 2

    def ccols(owner):
        return cotf.at[:, pl.ds(pl.multiple_of(owner * cshard, cshard), cshard)]

    def chalf(owner, half):
        tokens = pl.ds(pl.multiple_of(half * half_rows, half_rows), half_rows)
        return cotf.at[tokens, pl.ds(pl.multiple_of(owner * cshard, cshard), cshard)]

    def urgent(side):
        outer = side * (z_n - 1)
        return jnp.where(mz == outer, side * (z_n // 2) + 1 - side, outer)

    def other(side, quarter):
        return 2 * side * (z_n // 2) + 1 - quarter

    def cx_copy(order, src=None):
        quarter = urgent(mx) if order == 0 else other(mx, urgent(mx))
        ref = chalf(quarter, mc)
        return rcopy(ref if src is None else src, ref, c_send.at[order], c_recv.at[order], me, mirror)

    def cm_copy(order, half):
        quarter = urgent(1 - mx) if order == 0 else other(1 - mx, urgent(1 - mx))
        ref = chalf(quarter, half)
        return rcopy(ref, ref, c_send.at[2 + order], c_recv.at[2 + order], me, mate)

    part1, part2 = pl.ds(0, n1), pl.ds(n1, n2)

    def ag_copy(d, slot, part, zp):
        ref = wfull.at[drows(zp, 1 - my if part == 2 else my), part1 if part == 1 else part2]
        src = ref
        if slot == 0 and part < 2:
            src = w_hbm.at[:, part1 if part == 1 else part2]
        i = (d * z_n + slot) * 3 + part
        return rcopy(src, ref, ag_send.at[i], ag_recv.at[i], nxt[d], tp)

    def yw_copy(zp, own=False):
        ref = wfull.at[drows(zp, my), part1]
        return rcopy(w_hbm.at[:, part1] if own else ref, ref, yw_send.at[zp], yw_recv.at[zp], ynb, tp)

    def yw_wait(zp):
        ref = wfull.at[drows(zp, 1 - my), part1]
        rcopy(ref, ref, yw_send.at[zp], yw_recv.at[zp], ynb, tp).wait_recv()

    def rs_copy(d, slot, part, t):
        i = (d * z_n + slot) * 2 + part
        slot_to = z_n if d == 1 and slot == z_n - 1 else t
        src, dst = (sz2.at[t], rz2.at[slot_to]) if part == 0 else (sz1.at[t], rz1.at[slot_to])
        return rcopy(src, dst, rs_send.at[i], rs_recv.at[i], nxt[d], tp)

    def ry_copy(t):
        return rcopy(ysend.at[t], yrecv.at[t], ry_send.at[t], ry_recv.at[t], ynb, tp)

    own_w = pltpu.make_async_copy(w_hbm, wfull.at[drows(mz, my)], local_sem.at[0])
    own_c = pltpu.make_async_copy(cot_hbm, ccols(tp), local_sem.at[1])
    loads = [
        pltpu.make_async_copy(src, dst, local_sem.at[k])
        for k, (src, dst) in enumerate(
            [(up_hbm, ug_ref), (gate_hbm, gg_ref), (cw_hbm, cw_ref), (cb_hbm, cb_ref)], 2
        )
    ]

    barrier = pltpu.get_barrier_semaphore()
    peers = [((me + d) % fs_n, tp) for d in range(1, fs_n)] + [(me, mirror), (me, mate)]
    for peer in peers:
        pl.semaphore_signal(barrier, inc=1, device_id=peer, device_id_type=MESH)
    for copy in loads:
        copy.start()
    own_c.start()
    own_w.start()
    pl.semaphore_wait(barrier, len(peers))

    start(
        lambda: rcopy(up_hbm.at[pl.ds(rows - 16, 16)], halo_up, hu_sem.at[0], hu_sem.at[1], (me + 1) % fs_n, tp),
        me < fs_n - 1,
    )
    yp_copy = lambda: rcopy(
        w_hbm.at[:, part2], wfull.at[drows(mz, my), part2], yp_sem.at[0], yp_sem.at[1], ynb, tp
    )
    start(yp_copy)
    for part in (0, 1):
        for d in (0, 1):
            start(functools.partial(ag_copy, d, 0, part, mz), has_next[d])
    start(functools.partial(yw_copy, mz, True))
    start(lambda: rcopy(cot_hbm, ccols(tp), c_send.at[4], c_recv.at[4], me, mate))
    own_half = cot_hbm.at[pl.ds(pl.multiple_of(mc * half_rows, half_rows), half_rows)]
    leads = urgent(mx) == tp

    @pl.when(leads)
    def _():
        cx_copy(0, own_half).start()

    rcopy(cot_hbm, ccols(mate), c_send.at[4], c_recv.at[4], me, mate).wait_recv()

    @pl.when(leads)
    def _():
        cx_copy(1).start()

    @pl.when(jnp.logical_not(leads))
    def _():
        cx_copy(0).start()
        cx_copy(1, own_half).start()

    sends.append((None, functools.partial(cx_copy, 0)))
    sends.append((None, functools.partial(cx_copy, 1)))

    for copy in loads:
        copy.wait()

    upf[8 : rows + 8] = ug_ref[...].astype(F32)
    step = 64

    def conv_rows(first, end):
        @pl.loop(0, cols // 128)
        def _(j):
            lanes = pl.ds(pl.multiple_of(j * 128, 128), 128)
            taps = [cw_ref[k : k + 1, lanes] for k in range(3)]
            bias = cb_ref[0:1, lanes]
            for r in range(first, end, step):
                conv = bias + taps[0] * upf[r + 6 : r + 6 + step, lanes]
                conv = conv + taps[1] * upf[r + 7 : r + 7 + step, lanes]
                conv = conv + taps[2] * upf[r + 8 : r + 8 + step, lanes]
                sig = 1.0 / (1.0 + jnp.exp(-conv))
                a = conv * sig
                g = gg_ref[r : r + step, lanes].astype(F32)
                act[r : r + step, lanes] = a
                hidden[r : r + step, lanes] = (a * g).astype(BF16)
                gfac[r : r + step, lanes] = g * sig * (1.0 + conv * (1.0 - sig))

    conv_rows(step, rows)

    @pl.when(me > 0)
    def _():
        rcopy(halo_up, halo_up, hu_sem.at[0], hu_sem.at[1], (me + fs_n - 1) % fs_n, tp).wait_recv()
        upf[0:8] = halo_up[...].astype(F32)[8:16]

    @pl.when(me == 0)
    def _():
        upf[0:8] = jnp.zeros((8, cols), F32)

    conv_rows(0, step)

    rcopy(
        w_hbm.at[:, part2], wfull.at[drows(mz, 1 - my), part2], yp_sem.at[0], yp_sem.at[1], ynb, tp
    ).wait_recv()
    for d in (0, 1):
        start(functools.partial(ag_copy, d, 0, 2, mz), has_next[d])

    tile = min(256, cols)

    def wg_part(t):
        base = pl.multiple_of(t * ywide, ywide)
        lhs_t[...] = cotf[:, pl.ds(base, ywide)].T

        @pl.loop(0, cols // tile)
        def _(j):
            lanes = pl.ds(pl.multiple_of(j * tile, tile), tile)
            pf32[pl.ds(base, ywide), lanes] = jnp.dot(lhs_t[...], hidden[:, lanes], preferred_element_type=F32)

        @pl.loop(0, n1 // 128)
        def _(j):
            lanes = pl.ds(pl.multiple_of(j * 128, 128), 128)
            ysend[t, :, lanes] = pf32[drows(t, 1 - my), lanes].astype(BF16)

    first, second = urgent(mx), urgent(1 - mx)
    third, fourth = other(mx, first), other(1 - mx, second)

    def ry_start(t, delta=None):
        pred = None if delta is None else jnp.abs(t - mz) == delta
        start(functools.partial(ry_copy, t), pred)

    def wg_far(order):
        cx = fourth if order else second
        rcopy(chalf(cx, mc), chalf(cx, mc), c_send.at[order], c_recv.at[order], me, mirror).wait_recv()
        start(functools.partial(cm_copy, order, mc))
        cm_copy(order, 1 - mc).wait_recv()
        wg_part(cx)

    own_c.wait()
    wg_part(first)
    ry_start(first)
    wg_far(0)
    ry_start(second, z_n - 1)
    def ag_step(k, part):
        for d in (0, 1):
            zp = (mz + z_n - sign[d] * (1 + k)) % z_n
            is_ag = k < avail[d]

            @pl.when(is_ag)
            def _():
                ag_copy(d, k, part, zp).wait_recv()
                if k + 1 < z_n - 1:
                    @pl.when(has_next[d])
                    def _():
                        ag_copy(d, k + 1, part, zp).start()
                if part == 1:
                    yw_copy(zp).start()

            if k + 1 < z_n - 1:
                sends.append((is_ag & has_next[d], functools.partial(ag_copy, d, k + 1, part, zp)))
            if part == 1:
                sends.append((is_ag, functools.partial(yw_copy, zp)))

    def rs_step(k, part):
        for d in (0, 1):
            t = (mz + z_n - sign[d] * (1 + k)) % z_n
            pred = k >= avail[d]

            def run(arrived, d=d, t=t):
                if part == 1:
                    ry_copy(t).wait_recv()
                if arrived:
                    rs_copy(d, k, part, t).wait_recv()

                @pl.loop(0, (n1 if part else n2) // 128)
                def _(j):
                    near = pl.ds(pl.multiple_of(j * 128, 128), 128)
                    if part == 1:
                        total = pf32[drows(t, my), near] + yrecv[t, :, near].astype(F32)
                    else:
                        far = pl.ds(pl.multiple_of(n1 + j * 128, 128), 128)
                        total = pf32[pl.ds(pl.multiple_of(t * ywide, ywide), ywide), far]
                    if arrived:
                        total = total + (rz1 if part else rz2)[t, :, near].astype(F32)
                    (sz1 if part else sz2)[t, :, near] = total.astype(BF16)

                rs_copy(d, k + 1, part, t).start()

            if k > 0:
                pl.when(pred & has_prev[d])(functools.partial(run, True))
            pl.when(pred & jnp.logical_not(has_prev[d]))(functools.partial(run, False))
            sends.append((pred, functools.partial(rs_copy, d, k + 1, part, t)))

    part_rows = rows // 2 if rows % 32 == 0 else rows

    def hg_add(zp, first):
        base = pl.ds(pl.multiple_of(zp * ywide, ywide), ywide)

        @pl.loop(0, cols // tile)
        def _(j):
            lanes = pl.ds(pl.multiple_of(j * tile, tile), tile)

            @pl.loop(0, rows // part_rows)
            def _(i):
                part = pl.ds(pl.multiple_of(i * part_rows, part_rows), part_rows)
                hg = jnp.dot(cotf[part, base], wfull[base, lanes], preferred_element_type=F32)
                if not first:
                    hg = hg + cg[part, lanes]
                cg[part, lanes] = hg

    def hg_far(delta):
        for s in sign:
            zp = mz + s * delta

            @pl.when((zp >= 0) & (zp < z_n))
            def _():
                near = (zp + z_n) % z_n
                yw_wait(near)
                hg_add(near, False)

    ag_step(0, 0)
    ag_step(0, 1)
    for delta in range(z_n - 2, 1, -1):
        ry_start(second, delta)
    rs_step(0, 0)
    wg_part(third)
    for delta in range(z_n - 2, 1, -1):
        ry_start(third, delta)
    ag_step(0, 2)
    wg_far(1)
    for delta in range(z_n - 2, 1, -1):
        ry_start(fourth, delta)
    own_w.wait()
    yw_wait(mz)
    hg_add(mz, True)
    rs_step(0, 1)
    ag_step(1, 0)
    ag_step(1, 1)
    for t in (second, third, fourth):
        ry_start(t, 1)
    rs_step(1, 0)
    ag_step(1, 2)
    rs_step(1, 1)
    hg_far(1)
    ag_step(2, 0)
    ag_step(2, 1)
    for t in (second, third, fourth):
        ry_start(t, 0)
    rs_step(2, 0)
    ag_step(2, 2)
    rs_step(2, 1)
    hg_far(2)
    hg_far(z_n - 1)

    @pl.loop(0, cols // 128)
    def _(j):
        lanes = pl.ds(pl.multiple_of(j * 128, 128), 128)
        for r in range(0, rows, step):
            part = slice(r, r + step)
            hg = cg[part, lanes]
            gg_ref[part, lanes] = (hg * act[part, lanes]).astype(BF16)
            cg[part, lanes] = hg * gfac[part, lanes]

    start(
        lambda: rcopy(cg.at[pl.ds(0, 8)], halo_cg, hc_sem.at[0], hc_sem.at[1], (me + fs_n - 1) % fs_n, tp),
        me > 0,
    )

    @pl.loop(0, cols // 128)
    def _(j):
        lanes = pl.ds(pl.multiple_of(j * 128, 128), 128)
        sums = [jnp.zeros((8, 128), F32) for _ in range(4)]
        for r in range(0, rows, step):
            grad = cg[r : r + step, lanes]
            terms = [grad * upf[r + 6 + k : r + 6 + k + step, lanes] for k in range(3)] + [grad]
            sums = [s + jnp.sum(t.reshape(step // 8, 8, 128), axis=0) for s, t in zip(sums, terms)]
        for k in range(4):
            sy[my, k : k + 1, lanes] = jnp.sum(sums[k], axis=0, keepdims=True)

    start(lambda: rcopy(sy.at[my], sy.at[my], st_send.at[0], st_recv.at[z_n], ynb, tp))

    last = z_n - 1
    for d in (0, 1):

        @pl.when(has_prev[d])
        def _():
            rs_copy(d, last, 0, mz).wait_recv()

            @pl.loop(0, n2 // 128)
            def _(j):
                far = pl.ds(pl.multiple_of(n1 + j * 128, 128), 128)
                near = pl.ds(pl.multiple_of(j * 128, 128), 128)
                block = pl.ds(pl.multiple_of(mz * ywide, ywide), ywide)
                pf32[block, far] = pf32[block, far] + rz2[z_n if d == 1 else mz, :, near].astype(F32)

    @pl.loop(0, n2 // 128)
    def _(j):
        far = pl.ds(pl.multiple_of(n1 + j * 128, 128), 128)
        near = pl.ds(pl.multiple_of(j * 128, 128), 128)
        sf[:, near] = pf32[drows(mz, 1 - my), far].astype(BF16)

    f_copy = lambda: rcopy(sf, rf, f_sem.at[0], f_sem.at[1], ynb, tp)
    start(f_copy)

    rcopy(sy.at[1 - my], sy.at[1 - my], st_send.at[0], st_recv.at[z_n], ynb, tp).wait_recv()
    st[mz] = sy[0] + sy[1]
    for d in range(1, z_n):
        start(
            lambda d=d: rcopy(
                st.at[mz], st.at[mz], st_send.at[d], st_recv.at[mz], ((mz + d) % z_n) * y_n + my, tp
            )
        )

    own_block = drows(mz, my)
    ry_copy(mz).wait_recv()

    @pl.loop(0, n1 // 128)
    def _(j):
        lanes = pl.ds(pl.multiple_of(j * 128, 128), 128)
        wg_ref[:, lanes] = pf32[own_block, lanes] + yrecv[mz, :, lanes].astype(F32)

    for d in (0, 1):

        @pl.when(has_prev[d])
        def _():
            rs_copy(d, last, 1, mz).wait_recv()

            @pl.loop(0, n1 // 128)
            def _(j):
                lanes = pl.ds(pl.multiple_of(j * 128, 128), 128)
                wg_ref[:, lanes] = wg_ref[:, lanes] + rz1[z_n if d == 1 else mz, :, lanes].astype(F32)

    f_copy().wait_recv()

    @pl.loop(0, n2 // 128)
    def _(j):
        far = pl.ds(pl.multiple_of(n1 + j * 128, 128), 128)
        near = pl.ds(pl.multiple_of(j * 128, 128), 128)
        wg_ref[:, far] = pf32[own_block, far] + rf[:, near].astype(F32)

    @pl.loop(0, cols // 128)
    def _(j):
        lanes = pl.ds(pl.multiple_of(j * 128, 128), 128)
        total = wg_ref[:, lanes]
        nb[me, :, lanes] = jnp.sum(total * total, axis=0, keepdims=True)

    for d in range(1, fs_n):
        start(
            lambda d=d: rcopy(nb.at[me], nb.at[me], nb_send.at[d], nb_recv.at[me], (me + d) % fs_n, tp)
        )

    @pl.when(me < fs_n - 1)
    def _():
        rcopy(halo_cg, halo_cg, hc_sem.at[0], hc_sem.at[1], (me + 1) % fs_n, tp).wait_recv()
        cg[rows : rows + 8] = halo_cg[...]

    @pl.when(me == fs_n - 1)
    def _():
        cg[rows : rows + 8] = jnp.zeros((8, cols), F32)

    @pl.loop(0, cols // 128)
    def _(j):
        lanes = pl.ds(pl.multiple_of(j * 128, 128), 128)
        taps = [cw_ref[k : k + 1, lanes] for k in range(3)]
        for r in range(0, rows, step):
            total = taps[0] * cg[r + 2 : r + 2 + step, lanes]
            total = total + taps[1] * cg[r + 1 : r + 1 + step, lanes]
            total = total + taps[2] * cg[r : r + step, lanes]
            ug_ref[r : r + step, lanes] = total.astype(BF16)

    for d in range(1, z_n):
        zp = (mz + d) % z_n
        rcopy(st.at[zp], st.at[zp], st_send.at[d], st_recv.at[zp], zp * y_n + my, tp).wait_recv()
    stats = st[0]
    for d in range(1, z_n):
        stats = stats + st[d]
    tap_ref[...] = stats[0:3]
    bias_ref[...] = stats[3:4]

    for pred, make in sends:
        if pred is None:
            make().wait_send()
        else:
            @pl.when(pred)
            def _():
                make().wait_send()

    for d in range(1, fs_n):
        owner = (me + d) % fs_n
        rcopy(nb.at[owner], nb.at[owner], nb_send.at[d], nb_recv.at[owner], owner, tp).wait_recv()
    norms = nb[0]
    for k in range(1, fs_n):
        norms = norms + nb[k]
    norm_ref[...] = norms


def line_call(fs_n, tp_n, y_n, args):
    up_pre, _, _, down_weight, _, _ = args
    rows, cols = up_pre.shape
    dblk = down_weight.shape[0]
    width = dblk * fs_n
    ywide = y_n * dblk
    z_n = fs_n // y_n
    n2 = max(cols * 3 // 8 // 128, 1) * 128
    n1 = cols - n2
    dma = pltpu.SemaphoreType.DMA
    vmem = pl.BlockSpec(memory_space=pltpu.VMEM)
    return pl.pallas_call(
        functools.partial(line_kernel, fs_n, tp_n, y_n, n1),
        out_shape=(
            jax.ShapeDtypeStruct((rows, cols), BF16),
            jax.ShapeDtypeStruct((rows, cols), BF16),
            jax.ShapeDtypeStruct((dblk, cols), F32),
            jax.ShapeDtypeStruct((3, cols), F32),
            jax.ShapeDtypeStruct((1, cols), F32),
            jax.ShapeDtypeStruct((1, cols), F32),
        ),
        in_specs=[pl.BlockSpec(memory_space=pltpu.HBM)] * 6,
        out_specs=[vmem] * 6,
        scratch_shapes=[
            pltpu.VMEM((width, cols), BF16),
            pltpu.VMEM((rows, width), BF16),
            pltpu.VMEM((ywide, rows), BF16),
            pltpu.VMEM((rows, cols), BF16),
            pltpu.VMEM((rows, cols), F32),
            pltpu.VMEM((rows, cols), F32),
            pltpu.VMEM((rows + 8, cols), F32),
            pltpu.VMEM((rows + 8, cols), F32),
            pltpu.VMEM((width, cols), F32),
            pltpu.VMEM((z_n, dblk, n1), BF16),
            pltpu.VMEM((z_n, dblk, n1), BF16),
            pltpu.VMEM((z_n, dblk, n1), BF16),
            pltpu.VMEM((z_n + 1, dblk, n1), BF16),
            pltpu.VMEM((z_n, ywide, n2), BF16),
            pltpu.VMEM((z_n + 1, ywide, n2), BF16),
            pltpu.VMEM((dblk, n2), BF16),
            pltpu.VMEM((dblk, n2), BF16),
            pltpu.VMEM((y_n, 4, cols), F32),
            pltpu.VMEM((z_n, 4, cols), F32),
            pltpu.VMEM((fs_n, 1, cols), F32),
            pltpu.VMEM((16, cols), BF16),
            pltpu.VMEM((8, cols), F32),
            pltpu.VMEM((3, cols), F32),
            pltpu.VMEM((1, cols), F32),
            dma((6,)),
            dma((6 * z_n,)), dma((6 * z_n,)), dma((z_n,)), dma((z_n,)), dma((2,)),
            dma((5,)), dma((5,)), dma((z_n,)), dma((z_n,)),
            dma((4 * z_n,)), dma((4 * z_n,)), dma((2,)),
            dma((fs_n,)), dma((z_n,)), dma((fs_n,)), dma((fs_n,)),
            dma((2,)), dma((2,)),
        ],
        compiler_params=pltpu.CompilerParams(
            collective_id=0, has_side_effects=True, vmem_limit_bytes=46000 * 1024
        ),
    )(*args)


def write_kernel(*refs):
    count = len(refs) // 2
    sem = refs[-1]
    copies = [pltpu.make_async_copy(refs[k], refs[count + k], sem.at[k]) for k in range(count)]
    for copy in copies:
        copy.start()
    for copy in copies:
        copy.wait()


def write_out(values):
    return pl.pallas_call(
        write_kernel,
        out_shape=tuple(jax.ShapeDtypeStruct(v.shape, v.dtype) for v in values),
        in_specs=[pl.BlockSpec(memory_space=pltpu.VMEM)] * len(values),
        out_specs=[pl.BlockSpec(memory_space=pltpu.HBM)] * len(values),
        scratch_shapes=[pltpu.SemaphoreType.DMA((len(values),))],
        compiler_params=pltpu.CompilerParams(vmem_limit_bytes=1024 * 1024),
    )(*values)


def per_device(fs_n, tp_n, up_pre, gate_value, out_cotangent, down_weight, conv_weight, conv_bias):
    rows, cols = up_pre.shape
    dblk = down_weight.shape[0]
    width = dblk * fs_n
    y_n = max(tp_n // 2, 2)
    z_n = fs_n // y_n
    args = tuple(
        pltpu.with_memory_space_constraint(value, pltpu.HBM)
        for value in (up_pre, gate_value, out_cotangent, down_weight, conv_weight, conv_bias[None, :])
    )
    if tp_n == 4 and z_n == tp_n and rows % 64 == 0 and cols % 256 == 0 and dblk % 128 == 0:
        outs = write_out(line_call(fs_n, tp_n, y_n, args))
    else:
        outs = general_call(fs_n, tp_n, y_n, args)
    ug, gg, wg, tap, bias, norm = outs
    return ug, gg, wg, tap, bias[0], norm[0]


def solution(mesh):
    return jax.shard_map(
        functools.partial(per_device, mesh.shape["fs"], mesh.shape["tp"]),
        mesh=mesh,
        in_specs=(
            P("fs", "tp"),
            P("fs", "tp"),
            P("fs", "tp"),
            P("fs", "tp"),
            P(None, "tp"),
            P("tp"),
        ),
        out_specs=(P("fs", "tp"), P("fs", "tp"), P("fs", "tp"), P(None, "tp"), P("tp"), P("tp")),
        check_vma=False,
    )
```
